32 devices in a mesh: sp: 8 (over z, y), tp: 4 (over x, core).
Axes of the slice: x: 2, y: 2, z: 4, core: 2. Of those that a mesh axis runs over, the one named last changes fastest.
Arguments:
- query_rows: bfloat16 [4096, 1024], P('sp', 'tp'), may hold values from -6 to 6
- key_rows: bfloat16 [4096, 512], P('sp', 'tp'), may hold values from -6 to 6
- value_rows: bfloat16 [4096, 512], P('sp', 'tp'), may hold values from -12 to 12
- query_gain: float32 [128], replicated, may hold values from 0.2 to 6.5
- key_gain: float32 [128], replicated, may hold values from 0.2 to 6.5
- residual: bfloat16 [4096, 2048], P(('sp', 'tp')), may hold values from -6 to 6
- out_weight: bfloat16 [1024, 2048], P('tp'), may hold values from -3 to 3
- mix_gain: float32 [2048], replicated, may hold values from 0.1 to 1.9
- gate_weight: bfloat16 [2048, 5632], P('sp', 'tp'), may hold values from -0.125 to 0.125
- up_weight: bfloat16 [2048, 5632], P('sp', 'tp'), may hold values from -0.125 to 0.125
- down_weight: bfloat16 [5632, 2048], P('tp', 'sp'), may hold values from -0.15625 to 0.15625
Outputs:
- layer_out: bfloat16 [4096, 2048], P(('sp', 'tp'))
The draws below stay inside these ranges and needn't reach their ends.
All inputs are finite; a program needn't handle non-finite values.
Results may differ from the reference program's by a relative error of at most 0.015.
The reference program's roundings to bfloat16 on the way count: a program that leaves them out, or rounds other values in their place, can miss the bound.
Values may be sent and summed in bfloat16 or wider, within the bound.
A program may use at most 128 MiB of HBM per device.

```python
import jax
import jax.numpy as jnp
from jax import lax

D = 2048
HD = 128
QHEADS = 8
KVHEADS = 4
FF = 5632
GRID = 64
TOK_DEV = 512
TOKENS = 4096
N_TP = 4


def drawn_keys(key):
    base_keys = jnp.clip(jax.random.normal(jax.random.fold_in(key, 11), (TOKENS, KVHEADS * HD), jnp.float32), -6.0, 6.0)
    return base_keys


def draw_key_rows(key, part):
    return drawn_keys(key).astype(jnp.bfloat16)


def draw_query_rows(key, part):
    fresh = jnp.clip(jax.random.normal(jax.random.fold_in(key, 23), (TOKENS, QHEADS * HD), jnp.float32), -6.0, 6.0)
    return fresh.astype(jnp.bfloat16)


def gain_values(key):
    return 1.0 + 0.18 * jnp.clip(jax.random.normal(key, (HD,), jnp.float32), -4.4, 4.4)


def draw_query_gain(key, part):
    return gain_values(jax.random.fold_in(key, 31))


def draw_key_gain(key, part):
    return gain_values(jax.random.fold_in(key, 37))


def draw_out_weight(key, part):
    fresh = jnp.clip(jax.random.normal(jax.random.fold_in(key, 41), (QHEADS * HD, D), jnp.float32), -6.0, 6.0)
    spread = 0.5
    return (fresh * spread).astype(jnp.bfloat16)


def level_of(own_key, extent, pieces, least, largest):
    factor_of, own = 1.0, jax.random.fold_in(own_key, 6)
    for dim, shards_of in pieces:
        heights = jnp.exp(jax.random.uniform(jax.random.fold_in(own, dim), (shards_of,), jnp.float32, least / len(pieces), largest / len(pieces)))
        factor_of = factor_of * jnp.repeat(heights, extent[dim] // shards_of).reshape([-1 if axis == dim else 1 for axis in range(len(extent))])
    return factor_of


def bell_draw(own_key, dims, deviation, limit, cuts=(), kind=jnp.bfloat16):
    result = deviation * jax.random.normal(own_key, dims, jnp.float32)
    if cuts:
        result = result * level_of(own_key, dims, cuts, -0.22, 0.18)
    return jnp.clip(result, -limit, limit).astype(kind)


def setup_inputs(seed: int = 0) -> dict:
    keys = jax.random.split(jax.random.key(seed), 12)
    return {
        "query_rows": draw_query_rows(jax.random.fold_in(keys[11], 71), 0),
        "key_rows": draw_key_rows(jax.random.fold_in(keys[11], 71), 0),
        "value_rows": bell_draw(keys[2], (TOKENS, KVHEADS * HD), 2.0, 12.0, ((0, 8), (1, 4))),
        "query_gain": draw_query_gain(jax.random.fold_in(keys[11], 71), 0),
        "key_gain": draw_key_gain(jax.random.fold_in(keys[11], 71), 0),
        "residual": bell_draw(keys[5], (TOKENS, D), 1.0, 6.0, ((0, 32),)),
        "out_weight": draw_out_weight(jax.random.fold_in(keys[11], 71), 0),
        "mix_gain": jnp.clip(1.0 + 0.18 * jax.random.normal(keys[7], (D,), jnp.float32), 0.1, 1.9),
        "gate_weight": bell_draw(keys[8], (D, FF), D ** -0.5, 0.125, ((0, 8), (1, 4))),
        "up_weight": bell_draw(keys[9], (D, FF), D ** -0.5, 0.125, ((0, 8), (1, 4))),
        "down_weight": bell_draw(keys[10], (FF, D), (FF // 4) ** -0.5, 0.15625, ((0, 4), (1, 8))),
    }


norm_eps = 1e-06
theta_base = 10000.0

def spin(halfway, angles):
    cosine = jnp.cos(angles)[:, None, :]
    sine_val = jnp.sin(angles)[:, None, :]
    quarter = halfway.shape[-1] // 2
    leading = halfway[..., :quarter]
    trailing = halfway[..., quarter:]
    return [leading * cosine - trailing * sine_val, trailing * cosine + leading * sine_val]

def rotate_grid(vectors, positions):
    head_dim = vectors.shape[-1]
    quarter = head_dim // 4
    frequency = jnp.power(theta_base, -2.0 * jnp.arange(quarter, dtype=jnp.float32) / (head_dim // 2))
    row_angle = (positions // GRID).astype(jnp.float32)[:, None] * frequency
    col_angle = (positions % GRID).astype(jnp.float32)[:, None] * frequency
    lower_half = vectors[..., :2 * quarter]
    upper_half = vectors[..., 2 * quarter:]
    return jnp.concatenate(spin(lower_half, row_angle) + spin(upper_half, col_angle), axis=-1)

def prepare_heads(raw_heads, head_gain, positions):
    floated = raw_heads.astype(jnp.float32)
    scaled = floated * lax.rsqrt(lax.optimization_barrier(jnp.mean(floated * floated, axis=-1, keepdims=True)) + norm_eps)
    return rotate_grid(scaled * head_gain, positions).astype(jnp.bfloat16)

def row_norm(row_data, row_gain):
    floated = row_data.astype(jnp.float32)
    scaled = floated * lax.rsqrt(lax.optimization_barrier(jnp.mean(floated * floated, axis=-1, keepdims=True)) + norm_eps)
    return (scaled * row_gain).astype(jnp.bfloat16)

def to_wire(partial_value):
    return lax.optimization_barrier(partial_value.astype(jnp.bfloat16)).astype(jnp.float32)

def reference(query_rows, key_rows, value_rows, query_gain, key_gain, residual, out_weight, mix_gain, gate_weight, up_weight, down_weight):
    positions = jnp.arange(TOKENS, dtype=jnp.int32)
    group_size = QHEADS // KVHEADS
    q_heads = prepare_heads(query_rows.reshape(TOKENS, QHEADS, HD), query_gain, positions)
    k_heads = prepare_heads(key_rows.reshape(TOKENS, KVHEADS, HD), key_gain, positions).astype(jnp.float32)
    v_heads = value_rows.reshape(TOKENS, KVHEADS, HD).astype(jnp.float32)
    score_scale = HD ** (-0.5)
    q_blocks = q_heads.reshape(TOKENS // TOK_DEV, TOK_DEV, KVHEADS, group_size, HD)

    def attend(query_block):
        scores = jnp.einsum('qkgd,skd->kgqs', query_block.astype(jnp.float32), k_heads) * score_scale
        row_max = lax.optimization_barrier(jnp.max(scores, axis=-1, keepdims=True))
        weights = jnp.exp(scores - row_max)
        row_sum = lax.optimization_barrier(jnp.sum(weights, axis=-1))
        narrow = lax.optimization_barrier(weights.astype(jnp.bfloat16)).astype(jnp.float32)
        combined = jnp.einsum('kgqs,skd->qkgd', narrow, v_heads)
        return (combined / jnp.transpose(row_sum, (2, 0, 1))[..., None]).astype(jnp.bfloat16)
    attended = lax.map(attend, q_blocks).reshape(TOKENS, QHEADS * HD)
    head_cols = QHEADS * HD // N_TP
    attn_sum = jnp.zeros((TOKENS, D), jnp.float32)
    for member in range(N_TP):
        partial_value = jnp.dot(attended[:, member * head_cols:(member + 1) * head_cols], out_weight[member * head_cols:(member + 1) * head_cols], preferred_element_type=jnp.float32)
        attn_sum = attn_sum + to_wire(partial_value)
    updated = (residual.astype(jnp.float32) + attn_sum).astype(jnp.bfloat16)
    normed = row_norm(updated, mix_gain)
    unit_cols = FF // N_TP
    unit_sum = jnp.zeros((TOKENS, D), jnp.float32)
    for member in range(N_TP):
        gate_act = jnp.dot(normed, gate_weight[:, member * unit_cols:(member + 1) * unit_cols], preferred_element_type=jnp.float32)
        up_act = jnp.dot(normed, up_weight[:, member * unit_cols:(member + 1) * unit_cols], preferred_element_type=jnp.float32)
        hidden = (jax.nn.silu(gate_act) * up_act).astype(jnp.bfloat16)
        partial_value = jnp.dot(hidden, down_weight[member * unit_cols:(member + 1) * unit_cols], preferred_element_type=jnp.float32)
        unit_sum = unit_sum + to_wire(partial_value)
    return (updated.astype(jnp.float32) + 0.5 * unit_sum).astype(jnp.bfloat16)
```

```python
import functools
import math

import jax
import jax.numpy as jnp
import numpy as np
from jax import lax
from jax.experimental import pallas as pl
from jax.experimental.pallas import tpu as pltpu
from jax.sharding import PartitionSpec as P

GRID = 64

norm_eps = 1e-06
theta_base = 10000.0


def spin(halfway, angles):
    cosine = jnp.cos(angles)[:, None, :]
    sine_val = jnp.sin(angles)[:, None, :]
    quarter = halfway.shape[-1] // 2
    leading = halfway[..., :quarter]
    trailing = halfway[..., quarter:]
    return [leading * cosine - trailing * sine_val, trailing * cosine + leading * sine_val]


def rotate_grid(vectors, positions):
    head_dim = vectors.shape[-1]
    quarter = head_dim // 4
    frequency = jnp.power(
        theta_base, -2.0 * jnp.arange(quarter, dtype=jnp.float32) / (head_dim // 2)
    )
    row_angle = (positions // GRID).astype(jnp.float32)[:, None] * frequency
    col_angle = (positions % GRID).astype(jnp.float32)[:, None] * frequency
    lower_half = vectors[..., : 2 * quarter]
    upper_half = vectors[..., 2 * quarter :]
    return jnp.concatenate(spin(lower_half, row_angle) + spin(upper_half, col_angle), axis=-1)


def prepare_heads(raw_heads, head_gain, positions):
    floated = raw_heads.astype(jnp.float32)
    scaled = floated * lax.rsqrt(jnp.mean(floated * floated, axis=-1, keepdims=True) + norm_eps)
    return rotate_grid(scaled * head_gain, positions).astype(jnp.bfloat16)


def row_norm(row_data, row_gain):
    floated = row_data.astype(jnp.float32)
    scaled = floated * lax.rsqrt(jnp.mean(floated * floated, axis=-1, keepdims=True) + norm_eps)
    return (scaled * row_gain).astype(jnp.bfloat16)


def attend_body(factor, q_ref, k_ref, v_ref, o_ref):
    scores = lax.dot_general(
        q_ref[0], k_ref[0], (((1,), (1,)), ((), ())), preferred_element_type=jnp.float32
    )
    top = jnp.max(scores, axis=-1, keepdims=True)
    weights = jnp.exp2((scores - top) * factor)
    total = jnp.sum(weights, axis=-1, keepdims=True)
    mixed = jnp.dot(weights.astype(jnp.bfloat16), v_ref[0], preferred_element_type=jnp.float32)
    o_ref[0] = (mixed / total).astype(o_ref.dtype)


def attend(q_stack, keys, values):
    local_kv, rows, head_dim = q_stack.shape
    count = keys.shape[1]
    tile = min(256, rows)
    return pl.pallas_call(
        functools.partial(attend_body, head_dim**-0.5 * math.log2(math.e)),
        grid=(local_kv, rows // tile),
        in_specs=[
            pl.BlockSpec((1, tile, head_dim), lambda h, i: (h, i, 0)),
            pl.BlockSpec((1, count, head_dim), lambda h, i: (h, 0, 0)),
            pl.BlockSpec((1, count, head_dim), lambda h, i: (h, 0, 0)),
        ],
        out_specs=pl.BlockSpec((1, tile, head_dim), lambda h, i: (h, i, 0)),
        out_shape=jax.ShapeDtypeStruct((local_kv, rows, head_dim), jnp.bfloat16),
        compiler_params=pltpu.CompilerParams(vmem_limit_bytes=40 * 1024 * 1024),
        cost_estimate=pl.CostEstimate(
            flops=4 * local_kv * rows * count * head_dim,
            bytes_accessed=4 * local_kv * (rows + count) * head_dim,
            transcendentals=local_kv * rows * count,
        ),
    )(q_stack, keys, values)


def on_device(
    sp_size,
    tp_size,
    query_rows,
    key_rows,
    value_rows,
    query_gain,
    key_gain,
    residual,
    out_weight,
    mix_gain,
    gate_weight,
    up_weight,
    down_weight,
):
    ring = list(range(0, sp_size, 2)) + list(range(1, sp_size, 2))[::-1]
    onward = [(ring[i], ring[(i + 1) % sp_size]) for i in range(sp_size)]
    backward = [(b, a) for a, b in onward]
    sp_index, tp_index = lax.axis_index("sp"), lax.axis_index("tp")

    def travel(piece, perm, steps):
        out = []
        for _ in range(steps):
            piece = lax.ppermute(piece, "sp", perm)
            out.append(piece)
        return out

    def relabel(piece, rule):
        perm = []
        for s in range(sp_size):
            for t in range(tp_size):
                new_s, new_t = rule(s, t)
                if (new_s, new_t) == (s, t):
                    continue
                perm.append((s * tp_size + t, new_s * tp_size + new_t))
        return lax.ppermute(piece, ("sp", "tp"), perm)

    def flip(piece, sp_mask, tp_mask):
        return relabel(piece, lambda s, t: (s ^ sp_mask, t ^ tp_mask))

    def swap_bits(s, t):
        return (s & ~2) | ((t & 1) << 1), (t & ~1) | ((s >> 1) & 1)

    tok_rows = query_rows.shape[0]
    head_dim = query_gain.shape[0]
    local_kv = key_rows.shape[1] // head_dim
    local_q = query_rows.shape[1] // head_dim
    group_size = local_q // local_kv
    positions = lax.axis_index("sp") * tok_rows + jnp.arange(tok_rows, dtype=jnp.int32)

    k_heads = prepare_heads(
        key_rows.reshape(tok_rows, local_kv, head_dim), key_gain, positions
    ).reshape(tok_rows, local_kv * head_dim)
    kv = jnp.concatenate([k_heads, value_rows], axis=1)
    far = sp_size // 2
    kv_all = [kv] + travel(kv, onward, far) + travel(kv, backward, sp_size - 1 - far)

    bits = [1 << i for i in range(sp_size.bit_length() - 1)]
    order = bits[2:][::-1] + [1, 2]

    def collect(shard, gate_on):
        swapped = relabel(shard, swap_bits)
        keeps = ((sp_index >> 1) & 1) == (tp_index & 1)
        shard = jnp.where(keeps, shard, swapped)
        if gate_on is not None:
            shard, _ = lax.optimization_barrier((shard, gate_on))
        pieces = {0: shard}
        for bit in order:
            for mask in list(pieces):
                if bit == 2:
                    pieces[mask | bit] = flip(pieces[mask], 0, 1)
                else:
                    pieces[mask | bit] = flip(pieces[mask], bit, 0)
        return [pieces[mask] for mask in range(sp_size)]

    gate_on = (kv_all[far][:8], kv_all[-1][:8])
    gate_whole = jnp.concatenate(collect(gate_weight, gate_on), axis=0)
    up_whole = jnp.concatenate(collect(up_weight, gate_on), axis=0)
    down_whole = jnp.concatenate(collect(down_weight, gate_on), axis=1)

    q_heads = prepare_heads(query_rows.reshape(tok_rows, local_q, head_dim), query_gain, positions)
    q_stack = (
        q_heads.reshape(tok_rows, local_kv, group_size, head_dim)
        .transpose(1, 2, 0, 3)
        .reshape(local_kv, group_size * tok_rows, head_dim)
    )
    kv_whole = jnp.concatenate(kv_all, axis=0)
    kv_heads = kv_whole.reshape(sp_size * tok_rows, 2, local_kv, head_dim).transpose(1, 2, 0, 3)
    attended = attend(q_stack, kv_heads[0], kv_heads[1])
    attended = (
        attended.reshape(local_kv, group_size, tok_rows, head_dim)
        .transpose(2, 0, 1, 3)
        .reshape(tok_rows, local_q * head_dim)
    )
    own_count = tok_rows // tp_size
    by_peer = [
        lax.dynamic_slice_in_dim(attended, (tp_index ^ d) * own_count, own_count, 0)
        for d in range(tp_size)
    ]

    def summed(parts, masks):
        total = parts[0].astype(jnp.float32)
        arrived = [flip(piece, *mask) for piece, mask in zip(parts[1:], masks)]
        for piece in arrived:
            total = total + piece.astype(jnp.float32)
        return total

    def row_blocks(array):
        return [array[d * own_count : (d + 1) * own_count] for d in range(tp_size)]

    base = (sp_index & ~2) | ((tp_index & 1) << 1)
    width = down_weight.shape[1]

    def reorder(array):
        return jnp.concatenate(
            [
                lax.dynamic_slice_in_dim(array, (base ^ mask) * width, width, 1)
                for mask in range(sp_size)
            ],
            axis=1,
        )

    head_part = jnp.dot(
        jnp.concatenate(by_peer, axis=0), out_weight, preferred_element_type=jnp.float32
    ).astype(jnp.bfloat16)
    attn_sum = summed(row_blocks(head_part), [(0, d) for d in range(1, tp_size)])
    own_rows = (residual.astype(jnp.float32) + attn_sum).astype(jnp.bfloat16)
    group = [(0, 2), (2, 0), (2, 2)]
    normed = reorder(row_norm(own_rows, mix_gain))
    normed_all = jnp.concatenate([normed] + [flip(normed, *mask) for mask in group], axis=0)
    gate_act = jnp.dot(normed_all, gate_whole, preferred_element_type=jnp.float32)
    up_act = jnp.dot(normed_all, up_whole, preferred_element_type=jnp.float32)
    hidden = lax.optimization_barrier((jax.nn.silu(gate_act) * up_act).astype(jnp.bfloat16))
    unit_part = jnp.dot(hidden, down_whole, preferred_element_type=jnp.float32).astype(
        jnp.bfloat16
    )
    unit_sum = reorder(summed(row_blocks(unit_part), group))
    return (own_rows.astype(jnp.float32) + 0.5 * unit_sum).astype(jnp.bfloat16)


MESH = pl.DeviceIdType.MESH


def flip_bits(index, mask):
    out, step = index, 1
    while step <= mask:
        if mask & step:
            out = out + step * (1 - 2 * lax.rem(lax.div(index, step), 2))
        step *= 2
    return out


def turn(rows, gain, cosine, sine):
    count, head_dim = rows.shape
    quarter = head_dim // 4
    scaled = rows * lax.rsqrt(jnp.mean(rows * rows, axis=-1, keepdims=True) + norm_eps) * gain
    lane = lax.broadcasted_iota(jnp.int32, (count, head_dim), 1)
    paired = jnp.where(
        lax.rem(lane, 2 * quarter) < quarter,
        pltpu.roll(scaled, head_dim - quarter, 1),
        pltpu.roll(scaled, quarter, 1),
    )
    turned = scaled.reshape(cosine.shape) * cosine + paired.reshape(cosine.shape) * sine
    return turned.reshape(count, head_dim).astype(jnp.bfloat16)


def layer_body(
    sp_size,
    tp_size,
    q_ref,
    k_ref,
    v_ref,
    q_gain_ref,
    k_gain_ref,
    res_ref,
    ow_ref,
    mix_ref,
    gate_ref,
    up_ref,
    down_ref,
    row_cos_ref,
    row_sin_ref,
    col_cos_ref,
    col_sin_ref,
    out_ref,
    k_raw,
    v_all,
    k_all,
    q_raw,
    q_all,
    ow_all,
    gate_all,
    up_all,
    down_all,
    att,
    att_in,
    res,
    updated,
    normed,
    hidden,
    part,
    part_in,
    copy_sem,
    q_sem,
    q_out,
    w_sem,
    z_out,
    y_out,
    d_out,
    ow_sem,
    ow_out,
    ow_on,
    att_sem,
    att_out,
    norm_sem,
    norm_out,
    part_sem,
    part_out,
):
    sp, tp = lax.axis_index("sp"), lax.axis_index("tp")
    core = lax.rem(tp, 2)
    low = lax.rem(lax.div(sp, 2), 2)
    member = tp - core + low
    at_home = low == core
    tok_rows, head_dim = k_ref.shape
    own = tok_rows // tp_size
    heads = q_ref.shape[1] // head_dim
    depth, units = gate_ref.shape
    width = down_ref.shape[1]
    model = mix_ref.shape[1]
    group_rows = own * tp_size
    line = [m for m in range(2, sp_size, 2)]
    across = [m for m in range(1, sp_size, 2)]
    far = [m for m in range(4, sp_size, 4)]
    near = [m for m in range(2, sp_size, 4)]
    pending = []

    def remote(src, dst, out_sem, in_sem, sp_mask, tp_mask):
        return pltpu.make_async_remote_copy(
            src_ref=src,
            dst_ref=dst,
            send_sem=out_sem,
            recv_sem=in_sem,
            device_id=(flip_bits(sp, sp_mask), flip_bits(tp, tp_mask)),
            device_id_type=MESH,
        )

    def send(where, spec):
        remote(*spec()).start()
        pending.append((where, spec))

    def arrived(dst, sem):
        pltpu.make_async_copy(dst, dst, sem).wait()

    friends = (
        [(m, 0) for m in line]
        + [(1, 0), (0, 1), (2, 1)]
        + [(2 * (m & 1), m & ~1) for m in range(2, tp_size)]
    )
    barrier = pltpu.get_barrier_semaphore()
    for sp_mask, tp_mask in friends:
        pl.semaphore_signal(
            barrier,
            inc=1,
            device_id=(flip_bits(sp, sp_mask), flip_bits(tp, tp_mask)),
            device_id_type=MESH,
        )

    halves = 2
    chunks = [("k", 0, 0), ("v", 0, 0)]
    for half in range(halves):
        chunks += [("g", half, 0), ("u", half, 0)]
    for side in range(halves):
        for half in range(halves):
            chunks.append(("d", half, side))
    place = {name: i for i, name in enumerate(chunks)}

    def source(chunk):
        kind, half, side = chunk
        if kind in "kv":
            return k_ref if kind == "k" else v_ref
        if kind in "gu":
            ref = gate_ref if kind == "g" else up_ref
            return ref.at[pl.ds(half * (depth // halves), depth // halves)]
        return down_ref.at[
            pl.ds(half * (units // halves), units // halves),
            pl.ds(side * (width // halves), width // halves),
        ]

    def slot(chunk, shard):
        kind, half, side = chunk
        if kind in "kv":
            ref = k_raw if kind == "k" else v_all
            return ref.at[pl.ds(pl.multiple_of(shard * tok_rows, tok_rows), tok_rows)]
        if kind in "gu":
            ref = gate_all if kind == "g" else up_all
            rows = depth // halves
            return ref.at[pl.ds(pl.multiple_of(shard * depth + half * rows, rows), rows)]
        cols = width // halves
        rows = units // halves
        return down_all.at[
            side, pl.ds(half * rows, rows), pl.ds(pl.multiple_of(shard * cols, cols), cols)
        ]

    def own_spec(chunk, out_sem, sp_mask, tp_mask):
        in_sem = w_sem.at[place[chunk], sp]
        return source(chunk), slot(chunk, sp), out_sem, in_sem, sp_mask, tp_mask

    def along(chunk):
        n = place[chunk]

        @pl.when(at_home)
        def _():
            for i, mask in enumerate(far):
                send("home", lambda i=i, mask=mask: own_spec(chunk, z_out.at[n, i], mask, 0))

        @pl.when(jnp.logical_not(at_home))
        def _():
            for i, mask in enumerate(near):
                send("away", lambda i=i, mask=mask: own_spec(chunk, z_out.at[n, i], mask, 0))

    def settle(chunk):
        pltpu.make_async_copy(source(chunk), slot(chunk, sp), w_sem.at[place[chunk], sp]).start()

    def offer(chunk):
        n = place[chunk]

        @pl.when(at_home)
        def _():
            send("home", lambda: own_spec(chunk, y_out.at[n, 0], 1, 0))
            send("home", lambda: own_spec(chunk, d_out.at[n, 0], 0, 1))

    def relay(chunk, masks, over):
        n = place[chunk]
        for mask in masks:
            shard = flip_bits(sp, mask)
            arrived(slot(chunk, shard), w_sem.at[n, shard])

            def spec(out_sem, sp_mask, tp_mask, mask=mask):
                shard = flip_bits(sp, mask)
                here = slot(chunk, shard)
                return here, here, out_sem, w_sem.at[n, shard], sp_mask, tp_mask

            @pl.when(at_home)
            def _():
                if over:
                    send("home", lambda spec=spec, mask=mask: spec(y_out.at[n, mask // 2], 1, 0))
                send("home", lambda spec=spec, mask=mask: spec(d_out.at[n, mask], 0, 1))

    def lines(chunk):
        relay(chunk, line, True)

    def sides(chunk):
        arrived(slot(chunk, sp), w_sem.at[place[chunk], sp])
        relay(chunk, across, False)

    res_copy = pltpu.make_async_copy(res_ref, res, copy_sem)
    res_copy.start()
    ow_rows = ow_ref.shape[0]

    def ow_slot(index):
        return ow_all.at[pl.ds(pl.multiple_of(index * ow_rows, ow_rows), ow_rows)]

    pltpu.make_async_copy(ow_ref, ow_slot(tp), ow_sem.at[tp]).start()

    @pl.when(at_home)
    def _():
        for chunk in chunks:
            settle(chunk)

    pl.semaphore_wait(barrier, len(friends))

    for hi in range(tp_size // 2):
        for rel in range(2):

            def spec(sp_mask, tp_mask, hi=hi, rel=rel):
                mate = core + rel - 2 * core * rel
                src = q_ref.at[pl.ds(pl.multiple_of((2 * hi + mate) * own, own), own)]
                dst, sem = q_raw.at[2 * hi + low], q_sem.at[2 * hi + low]
                return src, dst, q_out.at[2 * hi + rel], sem, sp_mask, tp_mask

            @pl.when(at_home)
            def _():
                if rel == 0:
                    src, dst, _, sem, _, _ = spec(0, 0)
                    pltpu.make_async_copy(src, dst, sem).start()
                else:
                    send("home", lambda spec=spec: spec(0, 1))

            @pl.when(jnp.logical_not(at_home))
            def _():
                send("away", lambda spec=spec, rel=rel: spec(2, rel))

    kv = chunks[:2]
    rest = chunks[2:]
    for chunk in kv:
        along(chunk)
        offer(chunk)
    for hi in range(2, tp_size, 2):
        send(None, lambda hi=hi: (ow_ref, ow_slot(tp), ow_out.at[hi], ow_sem.at[tp], 0, hi))
    send(None, lambda: (ow_ref, ow_slot(tp), ow_out.at[0], ow_sem.at[tp], 0, 1))
    along(rest[0])
    along(rest[1])
    offer(rest[0])

    row_count = tok_rows // GRID

    def table(ref, col_ref, start, count):
        return ref[pl.ds(start, count), :][:, None, :] + col_ref[...][None]

    for m in range(tp_size):
        arrived(q_raw.at[m], q_sem.at[m])
        their_sp = sp - 2 * low + 2 * (m % 2)
        their_tp = 2 * (m // 2) + core
        own_grid = own // GRID
        start = (their_sp * tp_size + their_tp) * own_grid
        cosine = table(row_cos_ref, col_cos_ref, start, own_grid)
        sine = table(row_sin_ref, col_sin_ref, start, own_grid)
        for h in range(heads):
            raw = q_raw[m, :, h * head_dim : (h + 1) * head_dim].astype(jnp.float32)
            q_all[pl.ds(h * group_rows + m * own, own), :] = turn(
                raw, q_gain_ref[...], cosine, sine
            )

    def ready_keys(masks):
        for mask in masks:
            shard = flip_bits(sp, mask)
            rows = pl.ds(pl.multiple_of(shard * tok_rows, tok_rows), tok_rows)
            start = pl.multiple_of(shard * row_count, row_count)
            k_all[rows, :] = turn(
                k_raw[rows, :].astype(jnp.float32),
                k_gain_ref[...],
                table(row_cos_ref, col_cos_ref, start, row_count),
                table(row_sin_ref, col_sin_ref, start, row_count),
            )

    for chunk in kv:
        lines(chunk)
    ready_keys(line)
    for chunk in kv:
        sides(chunk)
    ready_keys([0] + across)

    along(rest[2])
    offer(rest[1])
    lines(rest[0])

    factor = head_dim**-0.5 * math.log2(math.e)
    tile = min(256, group_rows)
    per_head = group_rows // tile

    def attend_tile(i, carry):
        q_tile = q_all[pl.ds(pl.multiple_of(i * tile, tile), tile), :]
        scores = lax.dot_general(
            q_tile, k_all[...], (((1,), (1,)), ((), ())), preferred_element_type=jnp.float32
        )
        top = jnp.max(scores, axis=-1, keepdims=True)
        weights = jnp.exp2((scores - top) * factor)
        total = jnp.sum(weights, axis=-1, keepdims=True)
        mixed = jnp.dot(
            weights.astype(jnp.bfloat16), v_all[...], preferred_element_type=jnp.float32
        )
        head = lax.div(i, per_head)
        start = pl.multiple_of(lax.rem(i, per_head) * tile, tile)
        lanes = pl.ds(pl.multiple_of(head * head_dim, head_dim), head_dim)
        att[pl.ds(start, tile), lanes] = (mixed / total).astype(att.dtype)
        return carry

    lax.fori_loop(0, heads * per_head, attend_tile, 0)

    def rows_of(index):
        return pl.ds(pl.multiple_of(index * own, own), own)

    for m in range(1, tp_size):
        send(
            None,
            lambda m=m: (
                att.at[rows_of(flip_bits(member, m))],
                att_in.at[member],
                att_out.at[m],
                att_sem.at[member],
                2 * (m & 1),
                m & ~1,
            ),
        )
    att_in[member] = att[rows_of(member), :]

    along(rest[3])
    offer(rest[2])
    for hi in range(2, tp_size, 2):
        block = ow_slot(flip_bits(tp, hi))
        arrived(block, ow_sem.at[flip_bits(tp, hi)])

        def spec(hi=hi):
            index = flip_bits(tp, hi)
            return ow_slot(index), ow_slot(index), ow_on.at[hi], ow_sem.at[index], 0, 1

        send(None, spec)
    arrived(ow_slot(tp), ow_sem.at[tp])
    for hi in range(0, tp_size, 2):
        index = flip_bits(tp, hi + 1)
        arrived(ow_slot(index), ow_sem.at[index])
    res_copy.wait()
    for m in range(1, tp_size):
        arrived(att_in.at[flip_bits(member, m)], att_sem.at[flip_bits(member, m)])

    column = min(512, model)
    for start in range(0, model, column):
        lanes = slice(start, start + column)
        total = res[:, lanes].astype(jnp.float32)
        summed = None
        for m in range(tp_size):
            piece = (
                jnp.dot(
                    att_in[m],
                    ow_all[m * ow_rows : (m + 1) * ow_rows, lanes],
                    preferred_element_type=jnp.float32,
                )
                .astype(jnp.bfloat16)
                .astype(jnp.float32)
            )
            summed = piece if summed is None else summed + piece
        updated[:, lanes] = (total + summed).astype(jnp.bfloat16)
    floated = updated[...].astype(jnp.float32)
    scale = lax.rsqrt(jnp.mean(floated * floated, axis=-1, keepdims=True) + norm_eps)
    normed[rows_of(member), :] = (floated * scale * mix_ref[...]).astype(jnp.bfloat16)
    for m in range(1, tp_size):
        send(
            None,
            lambda m=m: (
                normed.at[rows_of(member)],
                normed.at[rows_of(member)],
                norm_out.at[m],
                norm_sem.at[member],
                2 * (m & 1),
                m & ~1,
            ),
        )

    sides(rest[0])
    lines(rest[1])
    along(rest[4])
    offer(rest[3])
    sides(rest[1])
    lines(rest[2])
    along(rest[5])
    offer(rest[4])
    sides(rest[2])
    lines(rest[3])
    along(rest[6])
    offer(rest[5])
    for m in range(1, tp_size):
        peer = flip_bits(member, m)
        arrived(normed.at[rows_of(peer)], norm_sem.at[peer])
    sides(rest[3])
    lines(rest[4])
    along(rest[7])
    offer(rest[6])

    unit_tile = 256
    starts = list(range(0, units, unit_tile))

    def feed(start):
        lanes = slice(start, min(start + unit_tile, units))
        gate = jnp.dot(normed[...], gate_all[:, lanes], preferred_element_type=jnp.float32)
        up = jnp.dot(normed[...], up_all[:, lanes], preferred_element_type=jnp.float32)
        hidden[:, lanes] = (gate / (1.0 + jnp.exp(-gate)) * up).astype(jnp.bfloat16)

    for n, start in enumerate(starts):
        feed(start)
        if n == 1:
            sides(rest[4])
            lines(rest[5])
            offer(rest[7])
    sides(rest[5])
    lines(rest[6])

    cols = sp_size * (width // halves)
    down_tile = min(256, cols)

    def project(side):
        for start in range(0, cols, down_tile):
            lanes = slice(start, start + down_tile)
            out = jnp.dot(hidden[...], down_all[side, :, lanes], preferred_element_type=jnp.float32)
            part[side, :, lanes] = out.astype(jnp.bfloat16)
        for m in range(1, tp_size):
            send(
                None,
                lambda m=m: (
                    part.at[side, rows_of(flip_bits(member, m))],
                    part_in.at[side, m - 1],
                    part_out.at[side, m],
                    part_sem.at[side, m],
                    2 * (m & 1),
                    m & ~1,
                ),
            )

    project(0)
    sides(rest[6])
    lines(rest[7])
    sides(rest[7])
    project(1)

    for side in range(halves):
        for m in range(1, tp_size):
            arrived(part_in.at[side, m - 1], part_sem.at[side, m])
        block = width // halves
        for shard in range(sp_size):
            lanes = slice(shard * block, (shard + 1) * block)
            total = part[side, rows_of(member), lanes].astype(jnp.float32)
            for m in range(1, tp_size):
                total = total + part_in[side, m - 1, :, lanes].astype(jnp.float32)
            there = slice(shard * width + side * block, shard * width + (side + 1) * block)
            out_ref[:, there] = (
                updated[:, there].astype(jnp.float32) + 0.5 * total
            ).astype(out_ref.dtype)

    for where, spec in pending:
        if where is None:
            remote(*spec()).wait_send()

    @pl.when(at_home)
    def _():
        for where, spec in pending:
            if where == "home":
                remote(*spec()).wait_send()

    @pl.when(jnp.logical_not(at_home))
    def _():
        for where, spec in pending:
            if where == "away":
                remote(*spec()).wait_send()


def grid_tables(rows, head_dim):
    quarter = head_dim // 4
    frequency = np.power(theta_base, -2.0 * np.arange(quarter) / (head_dim // 2)).astype(np.float32)

    def halves(count, first):
        angle = np.arange(count, dtype=np.float32)[:, None] * frequency
        cosine, sine = np.cos(angle.astype(np.float64)), np.sin(angle.astype(np.float64))
        empty = np.zeros((count, 2 * quarter))
        both = [np.concatenate([cosine, cosine], 1), np.concatenate([-sine, sine], 1)]
        return [
            np.concatenate([b, empty] if first else [empty, b], 1).astype(np.float32) for b in both
        ]

    return halves(rows, True) + halves(GRID, False)


def fused_device(
    sp_size,
    tp_size,
    query_rows,
    key_rows,
    value_rows,
    query_gain,
    key_gain,
    residual,
    out_weight,
    mix_gain,
    gate_weight,
    up_weight,
    down_weight,
):
    tok_rows, head_dim = key_rows.shape
    own = tok_rows // tp_size
    tokens = sp_size * tok_rows
    depth, units = gate_weight.shape
    model = mix_gain.shape[0]
    width = down_weight.shape[1]
    q_width = query_rows.shape[1]
    tables = grid_tables(tokens // GRID, head_dim)
    any_spec = pl.BlockSpec(memory_space=pl.ANY)
    vmem_spec = pl.BlockSpec(memory_space=pltpu.VMEM)
    dma = pltpu.SemaphoreType.DMA
    bf16 = jnp.bfloat16
    chunk_count = 10
    vm = pltpu.VMEM
    return pl.pallas_call(
        functools.partial(layer_body, sp_size, tp_size),
        out_shape=jax.ShapeDtypeStruct(residual.shape, residual.dtype),
        in_specs=[any_spec] * 3
        + [vmem_spec] * 2
        + [any_spec] * 2
        + [vmem_spec]
        + [any_spec] * 3
        + [vmem_spec] * 4,
        out_specs=vmem_spec,
        scratch_shapes=[
            vm((tokens, head_dim), bf16),
            vm((tokens, head_dim), bf16),
            vm((tokens, head_dim), bf16),
            vm((tp_size, own, q_width), bf16),
            vm((tok_rows * q_width // head_dim, head_dim), bf16),
            vm((tp_size * out_weight.shape[0], model), bf16),
            vm((sp_size * depth, units), bf16),
            vm((sp_size * depth, units), bf16),
            vm((2, units, sp_size * width // 2), bf16),
            vm((tok_rows, q_width), bf16),
            vm((tp_size, own, q_width), bf16),
            vm((own, model), bf16),
            vm((own, model), bf16),
            vm((tok_rows, model), bf16),
            vm((tok_rows, units), bf16),
            vm((2, tok_rows, sp_size * width // 2), bf16),
            vm((2, tp_size - 1, own, sp_size * width // 2), bf16),
            dma,
            dma((tp_size,)),
            dma((tp_size,)),
            dma((chunk_count, sp_size)),
            dma((chunk_count, sp_size // 4)),
            dma((chunk_count, sp_size // 2)),
            dma((chunk_count, sp_size)),
            dma((tp_size,)),
            dma((tp_size,)),
            dma((tp_size,)),
            dma((tp_size,)),
            dma((tp_size,)),
            dma((tp_size,)),
            dma((tp_size,)),
            dma((2, tp_size)),
            dma((2, tp_size)),
        ],
        compiler_params=pltpu.CompilerParams(
            collective_id=0, has_side_effects=True, vmem_limit_bytes=63 * 1024 * 1024
        ),
    )(
        query_rows,
        key_rows,
        value_rows,
        query_gain.reshape(1, -1),
        key_gain.reshape(1, -1),
        residual,
        out_weight,
        mix_gain.reshape(1, -1),
        gate_weight,
        up_weight,
        down_weight,
        *tables,
    )


def on_any_device(sp_size, tp_size, *args):
    query_rows, key_rows, _, query_gain, _, residual, _, _, gate_weight, _, down_weight = args
    lanes = query_gain.shape[0]
    tok_rows = key_rows.shape[0]
    whole = (
        key_rows.shape[1] == lanes
        and (down_weight.shape[1] // 2) % lanes == 0
        and gate_weight.shape[1] % lanes == 0
        and (tok_rows // tp_size) % GRID == 0
        and sp_size % 4 == 0
        and tp_size % 2 == 0
    )
    device = fused_device if whole else on_device
    return device(sp_size, tp_size, *args)


def solution(mesh):
    placed = (
        P("sp", "tp"),
        P("sp", "tp"),
        P("sp", "tp"),
        P(),
        P(),
        P(("sp", "tp"), None),
        P("tp", None),
        P(),
        P("sp", "tp"),
        P("sp", "tp"),
        P("tp", "sp"),
    )
    return jax.shard_map(
        functools.partial(on_any_device, mesh.shape["sp"], mesh.shape["tp"]),
        mesh=mesh,
        in_specs=placed,
        out_specs=P(("sp", "tp"), None),
        check_vma=False,
    )
```

```python
import functools
import math

import jax
import jax.numpy as jnp
import numpy as np
from jax import lax
from jax.experimental import pallas as pl
from jax.experimental.pallas import tpu as pltpu
from jax.sharding import PartitionSpec as P

GRID = 64

norm_eps = 1e-06
theta_base = 10000.0


def spin(halfway, angles):
    cosine = jnp.cos(angles)[:, None, :]
    sine_val = jnp.sin(angles)[:, None, :]
    quarter = halfway.shape[-1] // 2
    leading = halfway[..., :quarter]
    trailing = halfway[..., quarter:]
    return [leading * cosine - trailing * sine_val, trailing * cosine + leading * sine_val]


def rotate_grid(vectors, positions):
    head_dim = vectors.shape[-1]
    quarter = head_dim // 4
    frequency = jnp.power(
        theta_base, -2.0 * jnp.arange(quarter, dtype=jnp.float32) / (head_dim // 2)
    )
    row_angle = (positions // GRID).astype(jnp.float32)[:, None] * frequency
    col_angle = (positions % GRID).astype(jnp.float32)[:, None] * frequency
    lower_half = vectors[..., : 2 * quarter]
    upper_half = vectors[..., 2 * quarter :]
    return jnp.concatenate(spin(lower_half, row_angle) + spin(upper_half, col_angle), axis=-1)


def prepare_heads(raw_heads, head_gain, positions):
    floated = raw_heads.astype(jnp.float32)
    scaled = floated * lax.rsqrt(jnp.mean(floated * floated, axis=-1, keepdims=True) + norm_eps)
    return rotate_grid(scaled * head_gain, positions).astype(jnp.bfloat16)


def row_norm(row_data, row_gain):
    floated = row_data.astype(jnp.float32)
    scaled = floated * lax.rsqrt(jnp.mean(floated * floated, axis=-1, keepdims=True) + norm_eps)
    return (scaled * row_gain).astype(jnp.bfloat16)


def attend_body(factor, q_ref, k_ref, v_ref, o_ref):
    scores = lax.dot_general(
        q_ref[0], k_ref[0], (((1,), (1,)), ((), ())), preferred_element_type=jnp.float32
    )
    top = jnp.max(scores, axis=-1, keepdims=True)
    weights = jnp.exp2((scores - top) * factor)
    total = jnp.sum(weights, axis=-1, keepdims=True)
    mixed = jnp.dot(weights.astype(jnp.bfloat16), v_ref[0], preferred_element_type=jnp.float32)
    o_ref[0] = (mixed / total).astype(o_ref.dtype)


def attend(q_stack, keys, values):
    local_kv, rows, head_dim = q_stack.shape
    count = keys.shape[1]
    tile = min(256, rows)
    return pl.pallas_call(
        functools.partial(attend_body, head_dim**-0.5 * math.log2(math.e)),
        grid=(local_kv, rows // tile),
        in_specs=[
            pl.BlockSpec((1, tile, head_dim), lambda h, i: (h, i, 0)),
            pl.BlockSpec((1, count, head_dim), lambda h, i: (h, 0, 0)),
            pl.BlockSpec((1, count, head_dim), lambda h, i: (h, 0, 0)),
        ],
        out_specs=pl.BlockSpec((1, tile, head_dim), lambda h, i: (h, i, 0)),
        out_shape=jax.ShapeDtypeStruct((local_kv, rows, head_dim), jnp.bfloat16),
        compiler_params=pltpu.CompilerParams(vmem_limit_bytes=40 * 1024 * 1024),
        cost_estimate=pl.CostEstimate(
            flops=4 * local_kv * rows * count * head_dim,
            bytes_accessed=4 * local_kv * (rows + count) * head_dim,
            transcendentals=local_kv * rows * count,
        ),
    )(q_stack, keys, values)


def on_device(
    sp_size,
    tp_size,
    query_rows,
    key_rows,
    value_rows,
    query_gain,
    key_gain,
    residual,
    out_weight,
    mix_gain,
    gate_weight,
    up_weight,
    down_weight,
):
    ring = list(range(0, sp_size, 2)) + list(range(1, sp_size, 2))[::-1]
    onward = [(ring[i], ring[(i + 1) % sp_size]) for i in range(sp_size)]
    backward = [(b, a) for a, b in onward]
    sp_index, tp_index = lax.axis_index("sp"), lax.axis_index("tp")

    def travel(piece, perm, steps):
        out = []
        for _ in range(steps):
            piece = lax.ppermute(piece, "sp", perm)
            out.append(piece)
        return out

    def relabel(piece, rule):
        perm = []
        for s in range(sp_size):
            for t in range(tp_size):
                new_s, new_t = rule(s, t)
                if (new_s, new_t) == (s, t):
                    continue
                perm.append((s * tp_size + t, new_s * tp_size + new_t))
        return lax.ppermute(piece, ("sp", "tp"), perm)

    def flip(piece, sp_mask, tp_mask):
        return relabel(piece, lambda s, t: (s ^ sp_mask, t ^ tp_mask))

    def swap_bits(s, t):
        return (s & ~2) | ((t & 1) << 1), (t & ~1) | ((s >> 1) & 1)

    tok_rows = query_rows.shape[0]
    head_dim = query_gain.shape[0]
    local_kv = key_rows.shape[1] // head_dim
    local_q = query_rows.shape[1] // head_dim
    group_size = local_q // local_kv
    positions = lax.axis_index("sp") * tok_rows + jnp.arange(tok_rows, dtype=jnp.int32)

    k_heads = prepare_heads(
        key_rows.reshape(tok_rows, local_kv, head_dim), key_gain, positions
    ).reshape(tok_rows, local_kv * head_dim)
    kv = jnp.concatenate([k_heads, value_rows], axis=1)
    far = sp_size // 2
    kv_all = [kv] + travel(kv, onward, far) + travel(kv, backward, sp_size - 1 - far)

    bits = [1 << i for i in range(sp_size.bit_length() - 1)]
    order = bits[2:][::-1] + [1, 2]

    def collect(shard, gate_on):
        swapped = relabel(shard, swap_bits)
        keeps = ((sp_index >> 1) & 1) == (tp_index & 1)
        shard = jnp.where(keeps, shard, swapped)
        if gate_on is not None:
            shard, _ = lax.optimization_barrier((shard, gate_on))
        pieces = {0: shard}
        for bit in order:
            for mask in list(pieces):
                if bit == 2:
                    pieces[mask | bit] = flip(pieces[mask], 0, 1)
                else:
                    pieces[mask | bit] = flip(pieces[mask], bit, 0)
        return [pieces[mask] for mask in range(sp_size)]

    gate_on = (kv_all[far][:8], kv_all[-1][:8])
    gate_whole = jnp.concatenate(collect(gate_weight, gate_on), axis=0)
    up_whole = jnp.concatenate(collect(up_weight, gate_on), axis=0)
    down_whole = jnp.concatenate(collect(down_weight, gate_on), axis=1)

    q_heads = prepare_heads(query_rows.reshape(tok_rows, local_q, head_dim), query_gain, positions)
    q_stack = (
        q_heads.reshape(tok_rows, local_kv, group_size, head_dim)
        .transpose(1, 2, 0, 3)
        .reshape(local_kv, group_size * tok_rows, head_dim)
    )
    kv_whole = jnp.concatenate(kv_all, axis=0)
    kv_heads = kv_whole.reshape(sp_size * tok_rows, 2, local_kv, head_dim).transpose(1, 2, 0, 3)
    attended = attend(q_stack, kv_heads[0], kv_heads[1])
    attended = (
        attended.reshape(local_kv, group_size, tok_rows, head_dim)
        .transpose(2, 0, 1, 3)
        .reshape(tok_rows, local_q * head_dim)
    )
    own_count = tok_rows // tp_size
    by_peer = [
        lax.dynamic_slice_in_dim(attended, (tp_index ^ d) * own_count, own_count, 0)
        for d in range(tp_size)
    ]

    def summed(parts, masks):
        total = parts[0].astype(jnp.float32)
        arrived = [flip(piece, *mask) for piece, mask in zip(parts[1:], masks)]
        for piece in arrived:
            total = total + piece.astype(jnp.float32)
        return total

    def row_blocks(array):
        return [array[d * own_count : (d + 1) * own_count] for d in range(tp_size)]

    base = (sp_index & ~2) | ((tp_index & 1) << 1)
    width = down_weight.shape[1]

    def reorder(array):
        return jnp.concatenate(
            [
                lax.dynamic_slice_in_dim(array, (base ^ mask) * width, width, 1)
                for mask in range(sp_size)
            ],
            axis=1,
        )

    head_part = jnp.dot(
        jnp.concatenate(by_peer, axis=0), out_weight, preferred_element_type=jnp.float32
    ).astype(jnp.bfloat16)
    attn_sum = summed(row_blocks(head_part), [(0, d) for d in range(1, tp_size)])
    own_rows = (residual.astype(jnp.float32) + attn_sum).astype(jnp.bfloat16)
    group = [(0, 2), (2, 0), (2, 2)]
    normed = reorder(row_norm(own_rows, mix_gain))
    normed_all = jnp.concatenate([normed] + [flip(normed, *mask) for mask in group], axis=0)
    gate_act = jnp.dot(normed_all, gate_whole, preferred_element_type=jnp.float32)
    up_act = jnp.dot(normed_all, up_whole, preferred_element_type=jnp.float32)
    hidden = lax.optimization_barrier((jax.nn.silu(gate_act) * up_act).astype(jnp.bfloat16))
    unit_part = jnp.dot(hidden, down_whole, preferred_element_type=jnp.float32).astype(
        jnp.bfloat16
    )
    unit_sum = reorder(summed(row_blocks(unit_part), group))
    return (own_rows.astype(jnp.float32) + 0.5 * unit_sum).astype(jnp.bfloat16)


MESH = pl.DeviceIdType.MESH
AHEAD = 7
FIRST = 3
SECOND = 10
UNIT_TILE = 256
VMEM_LIMIT = 63 * 1024 * 1024


def flip_bits(index, mask):
    out, step = index, 1
    while step <= mask:
        if mask & step:
            out = out + step * (1 - 2 * lax.rem(lax.div(index, step), 2))
        step *= 2
    return out


def turn(rows, gain, cosine, sine):
    count, head_dim = rows.shape
    quarter = head_dim // 4
    scaled = rows * lax.rsqrt(jnp.mean(rows * rows, axis=-1, keepdims=True) + norm_eps) * gain
    lane = lax.broadcasted_iota(jnp.int32, (count, head_dim), 1)
    paired = jnp.where(
        lax.rem(lane, 2 * quarter) < quarter,
        pltpu.roll(scaled, head_dim - quarter, 1),
        pltpu.roll(scaled, quarter, 1),
    )
    turned = scaled.reshape(cosine.shape) * cosine + paired.reshape(cosine.shape) * sine
    return turned.reshape(count, head_dim).astype(jnp.bfloat16)


def layer_body(
    sp_size,
    tp_size,
    q_ref,
    k_ref,
    v_ref,
    q_gain_ref,
    k_gain_ref,
    res_ref,
    ow_ref,
    mix_ref,
    gate_ref,
    up_ref,
    down_ref,
    row_cos_ref,
    row_sin_ref,
    col_cos_ref,
    col_sin_ref,
    out_ref,
    k_raw,
    v_all,
    k_all,
    q_raw,
    q_all,
    ow_all,
    gate_all,
    up_all,
    down_all,
    att,
    att_in,
    res,
    updated,
    normed,
    hidden,
    part,
    part_in,
    summed_mate,
    copy_sem,
    q_sem,
    q_out,
    w_sem,
    z_out,
    y_out,
    d_out,
    ow_sem,
    ow_out,
    ow_on,
    att_sem,
    att_out,
    norm_sem,
    norm_out,
    part_sem,
    part_out,
):
    sp, tp = lax.axis_index("sp"), lax.axis_index("tp")
    core = lax.rem(tp, 2)
    low = lax.rem(lax.div(sp, 2), 2)
    member = tp - core + low
    at_home = low == core
    tok_rows, head_dim = k_ref.shape
    own = tok_rows // tp_size
    heads = q_ref.shape[1] // head_dim
    depth, units = gate_ref.shape
    width = down_ref.shape[1]
    model = mix_ref.shape[1]
    group_rows = own * tp_size
    line = [m for m in range(2, sp_size, 2)]
    across = [m for m in range(1, sp_size, 2)]
    far = [m for m in range(4, sp_size, 4)]
    near = [m for m in range(2, sp_size, 4)]
    pending = []

    def remote(src, dst, out_sem, in_sem, sp_mask, tp_mask):
        return pltpu.make_async_remote_copy(
            src_ref=src,
            dst_ref=dst,
            send_sem=out_sem,
            recv_sem=in_sem,
            device_id=(flip_bits(sp, sp_mask), flip_bits(tp, tp_mask)),
            device_id_type=MESH,
        )

    def send(where, spec):
        remote(*spec()).start()
        pending.append((where, spec))

    def drain(first, stop):
        def of(kind):
            for where, spec in pending[first:stop]:
                if where == kind:
                    remote(*spec()).wait_send()

        of(None)
        pl.when(at_home)(lambda: of("home"))
        pl.when(jnp.logical_not(at_home))(lambda: of("away"))

    def arrived(dst, sem):
        pltpu.make_async_copy(dst, dst, sem).wait()

    friends = (
        [(m, 0) for m in line]
        + [(1, 0), (0, 1), (2, 1)]
        + [(2 * (m & 1), m & ~1) for m in range(2, tp_size)]
    )
    barrier = pltpu.get_barrier_semaphore()
    for sp_mask, tp_mask in friends:
        pl.semaphore_signal(
            barrier,
            inc=1,
            device_id=(flip_bits(sp, sp_mask), flip_bits(tp, tp_mask)),
            device_id_type=MESH,
        )

    halves = 2
    chunks = [("k", 0, 0), ("v", 0, 0)]
    starts = list(range(0, units, UNIT_TILE))
    for start in starts:
        chunks += [("g", start, 0), ("u", start, 0)]
    for side in range(halves):
        for half in range(halves):
            chunks.append(("d", half, side))
    place = {name: i for i, name in enumerate(chunks)}

    def source(chunk):
        kind, half, side = chunk
        if kind in "kv":
            return k_ref if kind == "k" else v_ref
        if kind in "gu":
            ref = gate_ref if kind == "g" else up_ref
            return ref.at[:, pl.ds(half, min(UNIT_TILE, units - half))]
        return down_ref.at[
            pl.ds(half * (units // halves), units // halves),
            pl.ds(side * (width // halves), width // halves),
        ]

    def slot(chunk, shard):
        kind, half, side = chunk
        if kind in "kv":
            ref = k_raw if kind == "k" else v_all
            return ref.at[pl.ds(pl.multiple_of(shard * tok_rows, tok_rows), tok_rows)]
        if kind in "gu":
            ref = gate_all if kind == "g" else up_all
            rows = pl.ds(pl.multiple_of(shard * depth, depth), depth)
            return ref.at[rows, pl.ds(half, min(UNIT_TILE, units - half))]
        cols = width // halves
        rows = units // halves
        place_of = lax.rem(shard, 2) * (sp_size // 2) + lax.div(shard, 2)
        return down_all.at[
            side, pl.ds(half * rows, rows), pl.ds(pl.multiple_of(place_of * cols, cols), cols)
        ]

    def span(chunk, count):
        kind, half, side = chunk
        if kind in "kv":
            return k_raw.at[pl.ds(0, count * tok_rows)]
        if kind in "gu":
            return gate_all.at[pl.ds(0, count * depth), pl.ds(half, min(UNIT_TILE, units - half))]
        rows = pl.ds(0, units // halves)
        return down_all.at[side, rows, pl.ds(0, count * (width // halves))]

    def push(src, dst, out_sem, in_sem, sp_mask, tp_mask):
        remote(src, dst, out_sem, in_sem, sp_mask, tp_mask).start()

    def along(chunk):
        n = place[chunk]
        src, dst, sem = source(chunk), slot(chunk, sp), w_sem.at[n, sp]

        @pl.when(at_home)
        def _():
            for mask in far:
                push(src, dst, z_out.at[n], sem, mask, 0)

        @pl.when(jnp.logical_not(at_home))
        def _():
            for mask in near:
                push(src, dst, z_out.at[n], sem, mask, 0)

    def settle(chunk):
        pltpu.make_async_copy(source(chunk), slot(chunk, sp), w_sem.at[place[chunk], sp]).start()

    def offer(chunk):
        n = place[chunk]
        src, dst, sem = source(chunk), slot(chunk, sp), w_sem.at[n, sp]

        @pl.when(at_home)
        def _():
            push(src, dst, y_out.at[n], sem, 1, 0)
            push(src, dst, d_out.at[n], sem, 0, 1)

    def relay(chunk, masks, over):
        n = place[chunk]
        for mask in masks:
            shard = flip_bits(sp, mask)
            here, sem = slot(chunk, shard), w_sem.at[n, shard]
            arrived(here, sem)

            @pl.when(at_home)
            def _():
                if over:
                    push(here, here, y_out.at[n], sem, 1, 0)
                push(here, here, d_out.at[n], sem, 0, 1)

    def lines(chunk):
        relay(chunk, line, True)
        arrived(slot(chunk, sp), w_sem.at[place[chunk], sp])

    def sides(chunk, masks=across):
        relay(chunk, masks, False)

    def drain_weights():
        for n, chunk in enumerate(chunks):

            @pl.when(at_home)
            def _():
                if far:
                    arrived(span(chunk, len(far)), z_out.at[n])
                arrived(span(chunk, len(line) + 1), y_out.at[n])
                arrived(span(chunk, sp_size), d_out.at[n])

            @pl.when(jnp.logical_not(at_home))
            def _():
                arrived(span(chunk, len(near)), z_out.at[n])

    res_copy = pltpu.make_async_copy(res_ref, res, copy_sem)
    res_copy.start()
    ow_rows = ow_ref.shape[0]

    def ow_slot(index):
        return ow_all.at[pl.ds(pl.multiple_of(index * ow_rows, ow_rows), ow_rows)]

    pltpu.make_async_copy(ow_ref, ow_slot(tp), ow_sem.at[tp]).start()

    @pl.when(at_home)
    def _():
        for chunk in chunks:
            settle(chunk)

    pl.semaphore_wait(barrier, len(friends))

    for hi in range(tp_size // 2):
        for rel in range(2):

            def spec(sp_mask, tp_mask, hi=hi, rel=rel):
                mate = core + rel - 2 * core * rel
                src = q_ref.at[pl.ds(pl.multiple_of((2 * hi + mate) * own, own), own)]
                dst, sem = q_raw.at[2 * hi + low], q_sem.at[2 * hi + low]
                return src, dst, q_out.at[2 * hi + rel], sem, sp_mask, tp_mask

            @pl.when(at_home)
            def _():
                if rel == 0:
                    src, dst, _, sem, _, _ = spec(0, 0)
                    pltpu.make_async_copy(src, dst, sem).start()
                else:
                    send("home", lambda spec=spec: spec(0, 1))

            @pl.when(jnp.logical_not(at_home))
            def _():
                send("away", lambda spec=spec, rel=rel: spec(2, rel))

    kv = chunks[:2]
    rest = chunks[2:]
    for chunk in kv:
        along(chunk)
        offer(chunk)
    for hi in range(2, tp_size, 2):
        send(None, lambda hi=hi: (ow_ref, ow_slot(tp), ow_out.at[hi], ow_sem.at[tp], 0, hi))
    send(None, lambda: (ow_ref, ow_slot(tp), ow_out.at[0], ow_sem.at[tp], 0, 1))
    along(rest[0])
    for n in range(FIRST):
        offer(rest[n])

    def ahead(n):
        if n < len(rest):
            along(rest[n])

    row_count = tok_rows // GRID

    def table(ref, col_ref, start, count):
        return ref[pl.ds(start, count), :][:, None, :] + col_ref[...][None]

    for m in range(tp_size):
        arrived(q_raw.at[m], q_sem.at[m])
        their_sp = sp - 2 * low + 2 * (m % 2)
        their_tp = 2 * (m // 2) + core
        own_grid = own // GRID
        start = (their_sp * tp_size + their_tp) * own_grid
        cosine = table(row_cos_ref, col_cos_ref, start, own_grid)
        sine = table(row_sin_ref, col_sin_ref, start, own_grid)
        for h in range(heads):
            raw = q_raw[m, :, h * head_dim : (h + 1) * head_dim].astype(jnp.float32)
            q_all[pl.ds(h * group_rows + m * own, own), :] = turn(
                raw, q_gain_ref[...], cosine, sine
            )

    def ready_keys(masks):
        for mask in masks:
            shard = flip_bits(sp, mask)
            rows = pl.ds(pl.multiple_of(shard * tok_rows, tok_rows), tok_rows)
            start = pl.multiple_of(shard * row_count, row_count)
            k_all[rows, :] = turn(
                k_raw[rows, :].astype(jnp.float32),
                k_gain_ref[...],
                table(row_cos_ref, col_cos_ref, start, row_count),
                table(row_sin_ref, col_sin_ref, start, row_count),
            )

    for chunk in kv:
        lines(chunk)
    for n in range(FIRST, SECOND):
        offer(rest[n])
    for n in range(1, AHEAD):
        along(rest[n])
    ready_keys(line)
    for chunk in kv:
        sides(chunk)
    ready_keys([0] + across)

    for hi in range(2, tp_size, 2):
        block = ow_slot(flip_bits(tp, hi))
        arrived(block, ow_sem.at[flip_bits(tp, hi)])

        def spec(hi=hi):
            index = flip_bits(tp, hi)
            return ow_slot(index), ow_slot(index), ow_on.at[hi], ow_sem.at[index], 0, 1

        send(None, spec)
    lines(rest[0])

    factor = head_dim**-0.5 * math.log2(math.e)
    tile = min(256, group_rows)
    per_head = group_rows // tile

    def attend_tile(i, carry):
        q_tile = q_all[pl.ds(pl.multiple_of(i * tile, tile), tile), :]
        scores = lax.dot_general(
            q_tile, k_all[...], (((1,), (1,)), ((), ())), preferred_element_type=jnp.float32
        )
        top = jnp.max(scores, axis=-1, keepdims=True)
        weights = jnp.exp2((scores - top) * factor)
        total = jnp.sum(weights, axis=-1, keepdims=True)
        mixed = jnp.dot(
            weights.astype(jnp.bfloat16), v_all[...], preferred_element_type=jnp.float32
        )
        head = lax.div(i, per_head)
        start = pl.multiple_of(lax.rem(i, per_head) * tile, tile)
        lanes = pl.ds(pl.multiple_of(head * head_dim, head_dim), head_dim)
        att[pl.ds(start, tile), lanes] = (mixed / total).astype(att.dtype)
        return carry

    lax.fori_loop(0, heads * per_head, attend_tile, 0)

    def rows_of(index):
        return pl.ds(pl.multiple_of(index * own, own), own)

    for m in range(1, tp_size):
        send(
            None,
            lambda m=m: (
                att.at[rows_of(flip_bits(member, m))],
                att_in.at[member],
                att_out.at[m],
                att_sem.at[member],
                2 * (m & 1),
                m & ~1,
            ),
        )
    att_in[member] = att[rows_of(member), :]

    lines(rest[1])
    for n in range(SECOND, len(rest)):
        offer(rest[n])
    sides(rest[0])
    lines(rest[2])
    sides(rest[1])
    arrived(ow_slot(tp), ow_sem.at[tp])
    for hi in range(0, tp_size, 2):
        index = flip_bits(tp, hi + 1)
        arrived(ow_slot(index), ow_sem.at[index])
    res_copy.wait()
    for m in range(1, tp_size):
        arrived(att_in.at[flip_bits(member, m)], att_sem.at[flip_bits(member, m)])

    column = min(512, model)
    for start in range(0, model, column):
        lanes = slice(start, start + column)
        total = res[:, lanes].astype(jnp.float32)
        summed = None
        for m in range(tp_size):
            piece = (
                jnp.dot(
                    att_in[m],
                    ow_all[m * ow_rows : (m + 1) * ow_rows, lanes],
                    preferred_element_type=jnp.float32,
                )
                .astype(jnp.bfloat16)
                .astype(jnp.float32)
            )
            summed = piece if summed is None else summed + piece
        updated[:, lanes] = (total + summed).astype(jnp.bfloat16)
    floated = updated[...].astype(jnp.float32)
    scale = lax.rsqrt(jnp.mean(floated * floated, axis=-1, keepdims=True) + norm_eps)
    normed[rows_of(member), :] = (floated * scale * mix_ref[...]).astype(jnp.bfloat16)

    def normed_spec(index, out_sem, mask):
        rows = normed.at[rows_of(index)]
        return rows, rows, out_sem, norm_sem.at[index], 2 * (mask & 1), mask & ~1

    for m in [1] + list(range(2, tp_size, 2)):
        send(None, lambda m=m: normed_spec(member, norm_out.at[m], m))

    def normed_on():
        mate = flip_bits(member, 1)
        arrived(normed.at[rows_of(mate)], norm_sem.at[mate])
        for m in range(2, tp_size, 2):
            send(None, lambda m=m: normed_spec(flip_bits(member, 1), norm_out.at[m + 1], m))

    def feed(piece):
        lanes = slice(starts[piece], min(starts[piece] + UNIT_TILE, units))
        gate = jnp.dot(normed[...], gate_all[:, lanes], preferred_element_type=jnp.float32)
        up = jnp.dot(normed[...], up_all[:, lanes], preferred_element_type=jnp.float32)
        hidden[:, lanes] = (gate / (1.0 + jnp.exp(-gate)) * up).astype(jnp.bfloat16)

    weights = 2 * len(starts)
    fed = 0
    for n in range(AHEAD, AHEAD + 3):
        ahead(n)
    for n in range(3, weights):
        lines(rest[n])
        ahead(n + AHEAD)
        sides(rest[n - 1])
        if n == weights // 2:
            normed_on()
        if n == weights - 2:
            for m in range(2, tp_size):
                peer = flip_bits(member, m)
                arrived(normed.at[rows_of(peer)], norm_sem.at[peer])
        if n >= weights - 2:
            for _ in range(2):
                feed(fed)
                fed += 1
    lines(rest[weights])
    ahead(weights + AHEAD)
    sides(rest[weights - 1])
    for piece in range(fed, len(starts)):
        feed(piece)
    lines(rest[weights + 1])

    block = width // halves
    cols = sp_size // 2 * block
    y = lax.rem(sp, 2)
    down_tile = part.shape[-1]
    tiles = cols // down_tile
    in_tile = down_tile // block
    own_tile = lax.div(lax.div(sp, 2), in_tile)

    def project(side, half, tile):
        start = half * cols + tile * down_tile
        lanes = pl.ds(pl.multiple_of(start, down_tile), down_tile)
        out = jnp.dot(hidden[...], down_all[side, :, lanes], preferred_element_type=jnp.float32)
        part[side, half, tile] = out.astype(jnp.bfloat16)

    def give(side, half, order, mask, to, landing):
        def spec():
            return (
                part.at[side, half, :, rows_of(flip_bits(member, mask))],
                part_in.at[side, landing, half],
                part_out.at[side, mask, order],
                part_sem.at[side, landing, half, 0],
                2 * (to & 1),
                to & ~1,
            )

        send(None, spec)

    def give_all(side, half, order):
        for m in range(1, tp_size):
            give(side, half, order, m, m, m - 1)

    def give_tile(half, tile, order):
        for m in range(1, tp_size):

            def spec(m=m):
                return (
                    part.at[1, half, tile, rows_of(flip_bits(member, m))],
                    part_in.at[1, m - 1, half, tile],
                    part_out.at[1, m, order],
                    part_sem.at[1, m - 1, half, tile],
                    2 * (m & 1),
                    m & ~1,
                )

            send(None, spec)

    def give_up(half):
        for m in range(2, tp_size, 2):
            for low_mask in range(2):
                give(0, half, 0, m + low_mask, m, m + low_mask - 1)

    def give_down(half):
        for m in range(2, tp_size, 2):
            arrived(part_in.at[0, m, half], part_sem.at[0, m, half, 0])
        for tile in range(tiles):
            total = part[0, half, tile, rows_of(flip_bits(member, 1)), :].astype(jnp.float32)
            for m in range(2, tp_size, 2):
                total = total + part_in[0, m, half, tile].astype(jnp.float32)
            summed_mate[tile] = total.astype(jnp.bfloat16)
        send(
            None,
            lambda: (
                summed_mate,
                part_in.at[0, 0, half],
                part_out.at[0, 1, 0],
                part_sem.at[0, 0, half, 0],
                2,
                0,
            ),
        )

    def finish(side, half, landings, tile):
        total = part[side, half, tile, rows_of(member), :].astype(jnp.float32)
        for landing in landings:
            total = total + part_in[side, landing, half, tile].astype(jnp.float32)
        for n in range(in_tile):
            start = (2 * (tile * in_tile + n) + half) * width + side * block
            there = pl.ds(pl.multiple_of(start, block), block)
            out_ref[:, there] = (
                updated[:, there].astype(jnp.float32) + 0.5 * total[:, n * block : (n + 1) * block]
            ).astype(out_ref.dtype)

    def finish_half(side, half, landings):
        for landing in landings:
            arrived(part_in.at[side, landing, half], part_sem.at[side, landing, half, 0])
        for tile in range(tiles):
            finish(side, half, landings, tile)

    everyone = list(range(tp_size - 1))
    for tile in range(tiles):
        project(0, y, tile)
    give_up(y)
    sides(rest[weights])
    lines(rest[weights + 2])
    sides(rest[weights + 1])
    for tile in range(tiles):
        project(0, 1 - y, tile)
    give_all(0, 1 - y, 1)
    lines(rest[weights + 3])
    for tile in range(tiles):
        project(1, y, tile)
    give_all(1, y, 0)
    give_down(y)
    sides(rest[weights + 2])
    last = len(pending)
    for t in range(tiles):
        tile = flip_bits(own_tile, t)
        first = 2 * in_tile * t
        sides(rest[weights + 3], [m for m in across if first <= m < first + 2 * in_tile])
        project(1, 1 - y, tile)
        give_tile(1 - y, tile, 1 + t)
    drain_weights()
    drain(0, last)
    finish_half(0, y, [0] + [m - 1 for m in range(2, tp_size, 2)])
    finish_half(0, 1 - y, everyone)
    finish_half(1, y, everyone)
    for t in range(tiles):
        tile = flip_bits(own_tile, t)
        for landing in everyone:
            arrived(part_in.at[1, landing, 1 - y, tile], part_sem.at[1, landing, 1 - y, tile])
        finish(1, 1 - y, everyone, tile)
    drain(last, len(pending))


def grid_tables(rows, head_dim):
    quarter = head_dim // 4
    frequency = np.power(theta_base, -2.0 * np.arange(quarter) / (head_dim // 2)).astype(np.float32)

    def halves(count, first):
        angle = np.arange(count, dtype=np.float32)[:, None] * frequency
        cosine, sine = np.cos(angle.astype(np.float64)), np.sin(angle.astype(np.float64))
        empty = np.zeros((count, 2 * quarter))
        both = [np.concatenate([cosine, cosine], 1), np.concatenate([-sine, sine], 1)]
        return [
            np.concatenate([b, empty] if first else [empty, b], 1).astype(np.float32) for b in both
        ]

    return halves(rows, True) + halves(GRID, False)


def fused_device(
    sp_size,
    tp_size,
    query_rows,
    key_rows,
    value_rows,
    query_gain,
    key_gain,
    residual,
    out_weight,
    mix_gain,
    gate_weight,
    up_weight,
    down_weight,
):
    tok_rows, head_dim = key_rows.shape
    own = tok_rows // tp_size
    tokens = sp_size * tok_rows
    depth, units = gate_weight.shape
    model = mix_gain.shape[0]
    width = down_weight.shape[1]
    q_width = query_rows.shape[1]
    down_tile = min(256, sp_size * width // 4)
    tiles = sp_size * width // 4 // down_tile
    tables = grid_tables(tokens // GRID, head_dim)
    any_spec = pl.BlockSpec(memory_space=pltpu.HBM)
    vmem_spec = pl.BlockSpec(memory_space=pltpu.VMEM)
    dma = pltpu.SemaphoreType.DMA
    bf16 = jnp.bfloat16
    chunk_count = 2 + 2 * pl.cdiv(units, UNIT_TILE) + 4
    vm = pltpu.VMEM
    return pl.pallas_call(
        functools.partial(layer_body, sp_size, tp_size),
        out_shape=jax.ShapeDtypeStruct(residual.shape, residual.dtype),
        in_specs=[any_spec] * 3
        + [vmem_spec] * 2
        + [any_spec] * 2
        + [vmem_spec]
        + [any_spec] * 3
        + [vmem_spec] * 4,
        out_specs=vmem_spec,
        scratch_shapes=[
            vm((tokens, head_dim), bf16),
            vm((tokens, head_dim), bf16),
            vm((tokens, head_dim), bf16),
            vm((tp_size, own, q_width), bf16),
            vm((tok_rows * q_width // head_dim, head_dim), bf16),
            vm((tp_size * out_weight.shape[0], model), bf16),
            vm((sp_size * depth, units), bf16),
            vm((sp_size * depth, units), bf16),
            vm((2, units, sp_size * width // 2), bf16),
            vm((tok_rows, q_width), bf16),
            vm((tp_size, own, q_width), bf16),
            vm((own, model), bf16),
            vm((own, model), bf16),
            vm((tok_rows, model), bf16),
            vm((tok_rows, units), bf16),
            vm((2, 2, tiles, tok_rows, down_tile), bf16),
            vm((2, tp_size - 1, 2, tiles, own, down_tile), bf16),
            vm((tiles, own, down_tile), bf16),
            dma,
            dma((tp_size,)),
            dma((tp_size,)),
            dma((chunk_count, sp_size)),
            dma((chunk_count,)),
            dma((chunk_count,)),
            dma((chunk_count,)),
            dma((tp_size,)),
            dma((tp_size,)),
            dma((tp_size,)),
            dma((tp_size,)),
            dma((tp_size,)),
            dma((tp_size,)),
            dma((tp_size,)),
            dma((2, tp_size - 1, 2, tiles)),
            dma((2, tp_size, 1 + tiles)),
        ],
        compiler_params=pltpu.CompilerParams(
            collective_id=0, has_side_effects=True, vmem_limit_bytes=VMEM_LIMIT
        ),
    )(
        query_rows,
        key_rows,
        value_rows,
        query_gain.reshape(1, -1),
        key_gain.reshape(1, -1),
        residual,
        out_weight,
        mix_gain.reshape(1, -1),
        gate_weight,
        up_weight,
        down_weight,
        *tables,
    )


def on_any_device(sp_size, tp_size, *args):
    query_rows, key_rows, _, query_gain, _, residual, _, _, gate_weight, _, down_weight = args
    lanes = query_gain.shape[0]
    tok_rows = key_rows.shape[0]
    whole = (
        key_rows.shape[1] == lanes
        and (down_weight.shape[1] // 2) % lanes == 0
        and gate_weight.shape[1] % lanes == 0
        and (tok_rows // tp_size) % GRID == 0
        and sp_size % 4 == 0
        and tp_size % 2 == 0
    )
    device = fused_device if whole else on_device
    return device(sp_size, tp_size, *args)


def solution(mesh):
    placed = (
        P("sp", "tp"),
        P("sp", "tp"),
        P("sp", "tp"),
        P(),
        P(),
        P(("sp", "tp"), None),
        P("tp", None),
        P(),
        P("sp", "tp"),
        P("sp", "tp"),
        P("tp", "sp"),
    )
    return jax.shard_map(
        functools.partial(on_any_device, mesh.shape["sp"], mesh.shape["tp"]),
        mesh=mesh,
        in_specs=placed,
        out_specs=P(("sp", "tp"), None),
        check_vma=False,
    )
```

```python
import functools
import math

import jax
import jax.numpy as jnp
import numpy as np
from jax import lax
from jax.experimental import pallas as pl
from jax.experimental.pallas import tpu as pltpu
from jax.sharding import PartitionSpec as P

GRID = 64

norm_eps = 1e-06
theta_base = 10000.0


def spin(halfway, angles):
    cosine = jnp.cos(angles)[:, None, :]
    sine_val = jnp.sin(angles)[:, None, :]
    quarter = halfway.shape[-1] // 2
    leading = halfway[..., :quarter]
    trailing = halfway[..., quarter:]
    return [leading * cosine - trailing * sine_val, trailing * cosine + leading * sine_val]


def rotate_grid(vectors, positions):
    head_dim = vectors.shape[-1]
    quarter = head_dim // 4
    frequency = jnp.power(
        theta_base, -2.0 * jnp.arange(quarter, dtype=jnp.float32) / (head_dim // 2)
    )
    row_angle = (positions // GRID).astype(jnp.float32)[:, None] * frequency
    col_angle = (positions % GRID).astype(jnp.float32)[:, None] * frequency
    lower_half = vectors[..., : 2 * quarter]
    upper_half = vectors[..., 2 * quarter :]
    return jnp.concatenate(spin(lower_half, row_angle) + spin(upper_half, col_angle), axis=-1)


def prepare_heads(raw_heads, head_gain, positions):
    floated = raw_heads.astype(jnp.float32)
    scaled = floated * lax.rsqrt(jnp.mean(floated * floated, axis=-1, keepdims=True) + norm_eps)
    return rotate_grid(scaled * head_gain, positions).astype(jnp.bfloat16)


def row_norm(row_data, row_gain):
    floated = row_data.astype(jnp.float32)
    scaled = floated * lax.rsqrt(jnp.mean(floated * floated, axis=-1, keepdims=True) + norm_eps)
    return (scaled * row_gain).astype(jnp.bfloat16)


def attend_body(factor, q_ref, k_ref, v_ref, o_ref):
    scores = lax.dot_general(
        q_ref[0], k_ref[0], (((1,), (1,)), ((), ())), preferred_element_type=jnp.float32
    )
    top = jnp.max(scores, axis=-1, keepdims=True)
    weights = jnp.exp2((scores - top) * factor)
    total = jnp.sum(weights, axis=-1, keepdims=True)
    mixed = jnp.dot(weights.astype(jnp.bfloat16), v_ref[0], preferred_element_type=jnp.float32)
    o_ref[0] = (mixed / total).astype(o_ref.dtype)


def attend(q_stack, keys, values):
    local_kv, rows, head_dim = q_stack.shape
    count = keys.shape[1]
    tile = min(256, rows)
    return pl.pallas_call(
        functools.partial(attend_body, head_dim**-0.5 * math.log2(math.e)),
        grid=(local_kv, rows // tile),
        in_specs=[
            pl.BlockSpec((1, tile, head_dim), lambda h, i: (h, i, 0)),
            pl.BlockSpec((1, count, head_dim), lambda h, i: (h, 0, 0)),
            pl.BlockSpec((1, count, head_dim), lambda h, i: (h, 0, 0)),
        ],
        out_specs=pl.BlockSpec((1, tile, head_dim), lambda h, i: (h, i, 0)),
        out_shape=jax.ShapeDtypeStruct((local_kv, rows, head_dim), jnp.bfloat16),
        compiler_params=pltpu.CompilerParams(vmem_limit_bytes=40 * 1024 * 1024),
        cost_estimate=pl.CostEstimate(
            flops=4 * local_kv * rows * count * head_dim,
            bytes_accessed=4 * local_kv * (rows + count) * head_dim,
            transcendentals=local_kv * rows * count,
        ),
    )(q_stack, keys, values)


def on_device(
    sp_size,
    tp_size,
    query_rows,
    key_rows,
    value_rows,
    query_gain,
    key_gain,
    residual,
    out_weight,
    mix_gain,
    gate_weight,
    up_weight,
    down_weight,
):
    ring = list(range(0, sp_size, 2)) + list(range(1, sp_size, 2))[::-1]
    onward = [(ring[i], ring[(i + 1) % sp_size]) for i in range(sp_size)]
    backward = [(b, a) for a, b in onward]
    sp_index, tp_index = lax.axis_index("sp"), lax.axis_index("tp")

    def travel(piece, perm, steps):
        out = []
        for _ in range(steps):
            piece = lax.ppermute(piece, "sp", perm)
            out.append(piece)
        return out

    def relabel(piece, rule):
        perm = []
        for s in range(sp_size):
            for t in range(tp_size):
                new_s, new_t = rule(s, t)
                if (new_s, new_t) == (s, t):
                    continue
                perm.append((s * tp_size + t, new_s * tp_size + new_t))
        return lax.ppermute(piece, ("sp", "tp"), perm)

    def flip(piece, sp_mask, tp_mask):
        return relabel(piece, lambda s, t: (s ^ sp_mask, t ^ tp_mask))

    def swap_bits(s, t):
        return (s & ~2) | ((t & 1) << 1), (t & ~1) | ((s >> 1) & 1)

    tok_rows = query_rows.shape[0]
    head_dim = query_gain.shape[0]
    local_kv = key_rows.shape[1] // head_dim
    local_q = query_rows.shape[1] // head_dim
    group_size = local_q // local_kv
    positions = lax.axis_index("sp") * tok_rows + jnp.arange(tok_rows, dtype=jnp.int32)

    k_heads = prepare_heads(
        key_rows.reshape(tok_rows, local_kv, head_dim), key_gain, positions
    ).reshape(tok_rows, local_kv * head_dim)
    kv = jnp.concatenate([k_heads, value_rows], axis=1)
    far = sp_size // 2
    kv_all = [kv] + travel(kv, onward, far) + travel(kv, backward, sp_size - 1 - far)

    bits = [1 << i for i in range(sp_size.bit_length() - 1)]
    order = bits[2:][::-1] + [1, 2]

    def collect(shard, gate_on):
        swapped = relabel(shard, swap_bits)
        keeps = ((sp_index >> 1) & 1) == (tp_index & 1)
        shard = jnp.where(keeps, shard, swapped)
        if gate_on is not None:
            shard, _ = lax.optimization_barrier((shard, gate_on))
        pieces = {0: shard}
        for bit in order:
            for mask in list(pieces):
                if bit == 2:
                    pieces[mask | bit] = flip(pieces[mask], 0, 1)
                else:
                    pieces[mask | bit] = flip(pieces[mask], bit, 0)
        return [pieces[mask] for mask in range(sp_size)]

    gate_on = (kv_all[far][:8], kv_all[-1][:8])
    gate_whole = jnp.concatenate(collect(gate_weight, gate_on), axis=0)
    up_whole = jnp.concatenate(collect(up_weight, gate_on), axis=0)
    down_whole = jnp.concatenate(collect(down_weight, gate_on), axis=1)

    q_heads = prepare_heads(query_rows.reshape(tok_rows, local_q, head_dim), query_gain, positions)
    q_stack = (
        q_heads.reshape(tok_rows, local_kv, group_size, head_dim)
        .transpose(1, 2, 0, 3)
        .reshape(local_kv, group_size * tok_rows, head_dim)
    )
    kv_whole = jnp.concatenate(kv_all, axis=0)
    kv_heads = kv_whole.reshape(sp_size * tok_rows, 2, local_kv, head_dim).transpose(1, 2, 0, 3)
    attended = attend(q_stack, kv_heads[0], kv_heads[1])
    attended = (
        attended.reshape(local_kv, group_size, tok_rows, head_dim)
        .transpose(2, 0, 1, 3)
        .reshape(tok_rows, local_q * head_dim)
    )
    own_count = tok_rows // tp_size
    by_peer = [
        lax.dynamic_slice_in_dim(attended, (tp_index ^ d) * own_count, own_count, 0)
        for d in range(tp_size)
    ]

    def summed(parts, masks):
        total = parts[0].astype(jnp.float32)
        arrived = [flip(piece, *mask) for piece, mask in zip(parts[1:], masks)]
        for piece in arrived:
            total = total + piece.astype(jnp.float32)
        return total

    def row_blocks(array):
        return [array[d * own_count : (d + 1) * own_count] for d in range(tp_size)]

    base = (sp_index & ~2) | ((tp_index & 1) << 1)
    width = down_weight.shape[1]

    def reorder(array):
        return jnp.concatenate(
            [
                lax.dynamic_slice_in_dim(array, (base ^ mask) * width, width, 1)
                for mask in range(sp_size)
            ],
            axis=1,
        )

    head_part = jnp.dot(
        jnp.concatenate(by_peer, axis=0), out_weight, preferred_element_type=jnp.float32
    ).astype(jnp.bfloat16)
    attn_sum = summed(row_blocks(head_part), [(0, d) for d in range(1, tp_size)])
    own_rows = (residual.astype(jnp.float32) + attn_sum).astype(jnp.bfloat16)
    group = [(0, 2), (2, 0), (2, 2)]
    normed = reorder(row_norm(own_rows, mix_gain))
    normed_all = jnp.concatenate([normed] + [flip(normed, *mask) for mask in group], axis=0)
    gate_act = jnp.dot(normed_all, gate_whole, preferred_element_type=jnp.float32)
    up_act = jnp.dot(normed_all, up_whole, preferred_element_type=jnp.float32)
    hidden = lax.optimization_barrier((jax.nn.silu(gate_act) * up_act).astype(jnp.bfloat16))
    unit_part = jnp.dot(hidden, down_whole, preferred_element_type=jnp.float32).astype(
        jnp.bfloat16
    )
    unit_sum = reorder(summed(row_blocks(unit_part), group))
    return (own_rows.astype(jnp.float32) + 0.5 * unit_sum).astype(jnp.bfloat16)


MESH = pl.DeviceIdType.MESH
AHEAD = 7
FIRST = 3
SECOND = 10
UNIT_TILE = 256
VMEM_LIMIT = 63 * 1024 * 1024


def flip_bits(index, mask):
    out, step = index, 1
    while step <= mask:
        if mask & step:
            out = out + step * (1 - 2 * lax.rem(lax.div(index, step), 2))
        step *= 2
    return out


def turn(rows, gain, cosine, sine):
    count, head_dim = rows.shape
    quarter = head_dim // 4
    scaled = rows * lax.rsqrt(jnp.mean(rows * rows, axis=-1, keepdims=True) + norm_eps) * gain
    lane = lax.broadcasted_iota(jnp.int32, (count, head_dim), 1)
    paired = jnp.where(
        lax.rem(lane, 2 * quarter) < quarter,
        pltpu.roll(scaled, head_dim - quarter, 1),
        pltpu.roll(scaled, quarter, 1),
    )
    turned = scaled.reshape(cosine.shape) * cosine + paired.reshape(cosine.shape) * sine
    return turned.reshape(count, head_dim).astype(jnp.bfloat16)


def layer_body(
    sp_size,
    tp_size,
    q_ref,
    k_ref,
    v_ref,
    q_gain_ref,
    k_gain_ref,
    res_ref,
    ow_ref,
    mix_ref,
    gate_ref,
    up_ref,
    down_ref,
    row_cos_ref,
    row_sin_ref,
    col_cos_ref,
    col_sin_ref,
    out_ref,
    k_raw,
    v_all,
    k_all,
    q_raw,
    q_all,
    ow_all,
    gate_all,
    up_all,
    down_all,
    att,
    att_in,
    res,
    updated,
    normed,
    hidden,
    part,
    part_in,
    sums,
    copy_sem,
    q_sem,
    q_out,
    w_sem,
    z_out,
    y_out,
    d_out,
    ow_sem,
    ow_out,
    ow_on,
    att_sem,
    att_out,
    norm_sem,
    norm_out,
    part_sem,
    part_out,
    sum_out,
):
    sp, tp = lax.axis_index("sp"), lax.axis_index("tp")
    core = lax.rem(tp, 2)
    low = lax.rem(lax.div(sp, 2), 2)
    member = tp - core + low
    at_home = low == core
    tok_rows, head_dim = k_ref.shape
    own = tok_rows // tp_size
    heads = q_ref.shape[1] // head_dim
    depth, units = gate_ref.shape
    width = down_ref.shape[1]
    model = mix_ref.shape[1]
    group_rows = own * tp_size
    line = [m for m in range(2, sp_size, 2)]
    across = [m for m in range(1, sp_size, 2)]
    far = [m for m in range(4, sp_size, 4)]
    near = [m for m in range(2, sp_size, 4)]
    pending = []

    def remote(src, dst, out_sem, in_sem, sp_mask, tp_mask):
        return pltpu.make_async_remote_copy(
            src_ref=src,
            dst_ref=dst,
            send_sem=out_sem,
            recv_sem=in_sem,
            device_id=(flip_bits(sp, sp_mask), flip_bits(tp, tp_mask)),
            device_id_type=MESH,
        )

    def send(where, spec):
        remote(*spec()).start()
        pending.append((where, spec))

    def drain(first, stop):
        def of(kind):
            for where, spec in pending[first:stop]:
                if where == kind:
                    remote(*spec()).wait_send()

        of(None)
        pl.when(at_home)(lambda: of("home"))
        pl.when(jnp.logical_not(at_home))(lambda: of("away"))

    def arrived(dst, sem):
        pltpu.make_async_copy(dst, dst, sem).wait()

    friends = (
        [(m, 0) for m in line]
        + [(1, 0), (0, 1), (2, 1)]
        + [(2 * (m & 1), m & ~1) for m in range(2, tp_size)]
    )
    barrier = pltpu.get_barrier_semaphore()
    for sp_mask, tp_mask in friends:
        pl.semaphore_signal(
            barrier,
            inc=1,
            device_id=(flip_bits(sp, sp_mask), flip_bits(tp, tp_mask)),
            device_id_type=MESH,
        )

    halves = 2
    chunks = [("k", 0, 0), ("v", 0, 0)]
    starts = list(range(0, units, UNIT_TILE))
    for start in starts:
        chunks += [("g", start, 0), ("u", start, 0)]
    for side in range(halves):
        for half in range(halves):
            chunks.append(("d", half, side))
    place = {name: i for i, name in enumerate(chunks)}

    def source(chunk):
        kind, half, side = chunk
        if kind in "kv":
            return k_ref if kind == "k" else v_ref
        if kind in "gu":
            ref = gate_ref if kind == "g" else up_ref
            return ref.at[:, pl.ds(half, min(UNIT_TILE, units - half))]
        return down_ref.at[
            pl.ds(half * (units // halves), units // halves),
            pl.ds(side * (width // halves), width // halves),
        ]

    def slot(chunk, shard):
        kind, half, side = chunk
        if kind in "kv":
            ref = k_raw if kind == "k" else v_all
            return ref.at[pl.ds(pl.multiple_of(shard * tok_rows, tok_rows), tok_rows)]
        if kind in "gu":
            ref = gate_all if kind == "g" else up_all
            rows = pl.ds(pl.multiple_of(shard * depth, depth), depth)
            return ref.at[rows, pl.ds(half, min(UNIT_TILE, units - half))]
        cols = width // halves
        rows = units // halves
        place_of = lax.rem(shard, 2) * (sp_size // 2) + lax.div(shard, 2)
        return down_all.at[
            side, pl.ds(half * rows, rows), pl.ds(pl.multiple_of(place_of * cols, cols), cols)
        ]

    def bank(chunk):
        return "kvgud".index(chunk[0])

    def push(src, dst, out_sem, in_sem, sp_mask, tp_mask):
        remote(src, dst, out_sem, in_sem, sp_mask, tp_mask).start()

    def along(chunk):
        n = place[chunk]
        src, dst, sem = source(chunk), slot(chunk, sp), w_sem.at[n, sp]

        @pl.when(at_home)
        def _():
            for mask in far:
                push(src, dst, z_out.at[bank(chunk)], sem, mask, 0)

        @pl.when(jnp.logical_not(at_home))
        def _():
            for mask in near:
                push(src, dst, z_out.at[bank(chunk)], sem, mask, 0)

    def settle(chunk):
        pltpu.make_async_copy(source(chunk), slot(chunk, sp), w_sem.at[place[chunk], sp]).start()

    def offer(chunk):
        n = place[chunk]
        src, dst, sem = source(chunk), slot(chunk, sp), w_sem.at[n, sp]

        @pl.when(at_home)
        def _():
            push(src, dst, y_out.at[bank(chunk)], sem, 1, 0)
            push(src, dst, d_out.at[bank(chunk)], sem, 0, 1)

    def relay(chunk, masks, over):
        n = place[chunk]
        for mask in masks:
            shard = flip_bits(sp, mask)
            here, sem = slot(chunk, shard), w_sem.at[n, shard]
            arrived(here, sem)

            @pl.when(at_home)
            def _():
                if over:
                    push(here, here, y_out.at[bank(chunk)], sem, 1, 0)
                push(here, here, d_out.at[bank(chunk)], sem, 0, 1)

    def lines(chunk):
        relay(chunk, line, True)
        arrived(slot(chunk, sp), w_sem.at[place[chunk], sp])

    def sides(chunk, masks=across):
        relay(chunk, masks, False)

    def drain_weights():
        def spans(count):
            for name, ref in enumerate((k_raw, v_all)):
                yield name, ref.at[pl.ds(0, count * tok_rows)]
            for name, ref in enumerate((gate_all, up_all)):
                yield 2 + name, ref.at[pl.ds(0, count * depth)]
            yield 4, down_all.at[:, :, pl.ds(0, count * (width // halves))]

        def wait(sem, count):
            for name, ref in spans(count):
                arrived(ref, sem.at[name])

        @pl.when(at_home)
        def _():
            if far:
                wait(z_out, len(far))
            wait(y_out, len(line) + 1)
            wait(d_out, sp_size)

        @pl.when(jnp.logical_not(at_home))
        def _():
            wait(z_out, len(near))

    res_copy = pltpu.make_async_copy(res_ref, res, copy_sem)
    res_copy.start()
    ow_rows = ow_ref.shape[0]

    def ow_slot(index):
        return ow_all.at[pl.ds(pl.multiple_of(index * ow_rows, ow_rows), ow_rows)]

    pltpu.make_async_copy(ow_ref, ow_slot(tp), ow_sem.at[tp]).start()

    @pl.when(at_home)
    def _():
        for chunk in chunks:
            settle(chunk)

    pl.semaphore_wait(barrier, len(friends))

    for hi in range(tp_size // 2):
        for rel in range(2):

            def spec(sp_mask, tp_mask, hi=hi, rel=rel):
                mate = core + rel - 2 * core * rel
                src = q_ref.at[pl.ds(pl.multiple_of((2 * hi + mate) * own, own), own)]
                dst, sem = q_raw.at[2 * hi + low], q_sem.at[2 * hi + low]
                return src, dst, q_out.at[2 * hi + rel], sem, sp_mask, tp_mask

            @pl.when(at_home)
            def _():
                if rel == 0:
                    src, dst, _, sem, _, _ = spec(0, 0)
                    pltpu.make_async_copy(src, dst, sem).start()
                else:
                    send("home", lambda spec=spec: spec(0, 1))

            @pl.when(jnp.logical_not(at_home))
            def _():
                send("away", lambda spec=spec, rel=rel: spec(2, rel))

    kv = chunks[:2]
    rest = chunks[2:]
    for chunk in kv:
        along(chunk)
        offer(chunk)
    for hi in range(2, tp_size, 2):
        send(None, lambda hi=hi: (ow_ref, ow_slot(tp), ow_out.at[hi], ow_sem.at[tp], 0, hi))
    send(None, lambda: (ow_ref, ow_slot(tp), ow_out.at[0], ow_sem.at[tp], 0, 1))
    along(rest[0])
    for n in range(FIRST):
        offer(rest[n])

    def ahead(n):
        if n < len(rest):
            along(rest[n])

    row_count = tok_rows // GRID

    def table(ref, col_ref, start, count):
        return ref[pl.ds(start, count), :][:, None, :] + col_ref[...][None]

    for m in range(tp_size):
        arrived(q_raw.at[m], q_sem.at[m])
        their_sp = sp - 2 * low + 2 * (m % 2)
        their_tp = 2 * (m // 2) + core
        own_grid = own // GRID
        start = (their_sp * tp_size + their_tp) * own_grid
        cosine = table(row_cos_ref, col_cos_ref, start, own_grid)
        sine = table(row_sin_ref, col_sin_ref, start, own_grid)
        for h in range(heads):
            raw = q_raw[m, :, h * head_dim : (h + 1) * head_dim].astype(jnp.float32)
            q_all[pl.ds(h * group_rows + m * own, own), :] = turn(
                raw, q_gain_ref[...], cosine, sine
            )

    def ready_keys(masks):
        for mask in masks:
            shard = flip_bits(sp, mask)
            rows = pl.ds(pl.multiple_of(shard * tok_rows, tok_rows), tok_rows)
            start = pl.multiple_of(shard * row_count, row_count)
            k_all[rows, :] = turn(
                k_raw[rows, :].astype(jnp.float32),
                k_gain_ref[...],
                table(row_cos_ref, col_cos_ref, start, row_count),
                table(row_sin_ref, col_sin_ref, start, row_count),
            )

    for chunk in kv:
        lines(chunk)
    for n in range(FIRST, SECOND):
        offer(rest[n])
    for n in range(1, AHEAD):
        along(rest[n])
    ready_keys(line)
    for chunk in kv:
        sides(chunk)
    ready_keys([0] + across)

    for hi in range(2, tp_size, 2):
        block = ow_slot(flip_bits(tp, hi))
        arrived(block, ow_sem.at[flip_bits(tp, hi)])

        def spec(hi=hi):
            index = flip_bits(tp, hi)
            return ow_slot(index), ow_slot(index), ow_on.at[hi], ow_sem.at[index], 0, 1

        send(None, spec)
    lines(rest[0])

    factor = head_dim**-0.5 * math.log2(math.e)
    tile = min(256, group_rows)
    per_head = group_rows // tile

    def attend_tile(i, carry):
        q_tile = q_all[pl.ds(pl.multiple_of(i * tile, tile), tile), :]
        scores = lax.dot_general(
            q_tile, k_all[...], (((1,), (1,)), ((), ())), preferred_element_type=jnp.float32
        )
        top = jnp.max(scores, axis=-1, keepdims=True)
        weights = jnp.exp2((scores - top) * factor)
        total = jnp.sum(weights, axis=-1, keepdims=True)
        mixed = jnp.dot(
            weights.astype(jnp.bfloat16), v_all[...], preferred_element_type=jnp.float32
        )
        head = lax.div(i, per_head)
        start = pl.multiple_of(lax.rem(i, per_head) * tile, tile)
        lanes = pl.ds(pl.multiple_of(head * head_dim, head_dim), head_dim)
        att[pl.ds(start, tile), lanes] = (mixed / total).astype(att.dtype)
        return carry

    lax.fori_loop(0, heads * per_head, attend_tile, 0)

    def rows_of(index):
        return pl.ds(pl.multiple_of(index * own, own), own)

    for m in range(1, tp_size):
        send(
            None,
            lambda m=m: (
                att.at[rows_of(flip_bits(member, m))],
                att_in.at[member],
                att_out.at[m],
                att_sem.at[member],
                2 * (m & 1),
                m & ~1,
            ),
        )
    att_in[member] = att[rows_of(member), :]

    lines(rest[1])
    for n in range(SECOND, len(rest)):
        offer(rest[n])
    sides(rest[0])
    lines(rest[2])
    sides(rest[1])
    arrived(ow_slot(tp), ow_sem.at[tp])
    for hi in range(0, tp_size, 2):
        index = flip_bits(tp, hi + 1)
        arrived(ow_slot(index), ow_sem.at[index])
    res_copy.wait()
    for m in range(1, tp_size):
        arrived(att_in.at[flip_bits(member, m)], att_sem.at[flip_bits(member, m)])

    column = min(512, model)
    for start in range(0, model, column):
        lanes = slice(start, start + column)
        total = res[:, lanes].astype(jnp.float32)
        summed = None
        for m in range(tp_size):
            piece = (
                jnp.dot(
                    att_in[m],
                    ow_all[m * ow_rows : (m + 1) * ow_rows, lanes],
                    preferred_element_type=jnp.float32,
                )
                .astype(jnp.bfloat16)
                .astype(jnp.float32)
            )
            summed = piece if summed is None else summed + piece
        updated[:, lanes] = (total + summed).astype(jnp.bfloat16)
    floated = updated[...].astype(jnp.float32)
    scale = lax.rsqrt(jnp.mean(floated * floated, axis=-1, keepdims=True) + norm_eps)
    normed[rows_of(member), :] = (floated * scale * mix_ref[...]).astype(jnp.bfloat16)

    def normed_spec(index, out_sem, mask):
        rows = normed.at[rows_of(index)]
        return rows, rows, out_sem, norm_sem.at[index], 2 * (mask & 1), mask & ~1

    for m in [1] + list(range(2, tp_size, 2)):
        send(None, lambda m=m: normed_spec(member, norm_out.at[m], m))

    def normed_on():
        mate = flip_bits(member, 1)
        arrived(normed.at[rows_of(mate)], norm_sem.at[mate])
        for m in range(2, tp_size, 2):
            send(None, lambda m=m: normed_spec(flip_bits(member, 1), norm_out.at[m + 1], m))

    def feed(piece):
        lanes = slice(starts[piece], min(starts[piece] + UNIT_TILE, units))
        gate = jnp.dot(normed[...], gate_all[:, lanes], preferred_element_type=jnp.float32)
        up = jnp.dot(normed[...], up_all[:, lanes], preferred_element_type=jnp.float32)
        hidden[:, lanes] = (gate / (1.0 + jnp.exp(-gate)) * up).astype(jnp.bfloat16)

    weights = 2 * len(starts)
    fed = 0
    for n in range(AHEAD, AHEAD + 3):
        ahead(n)
    for n in range(3, weights):
        lines(rest[n])
        ahead(n + AHEAD)
        sides(rest[n - 1])
        if n == weights // 2:
            normed_on()
        if n == weights - 2:
            for m in range(2, tp_size):
                peer = flip_bits(member, m)
                arrived(normed.at[rows_of(peer)], norm_sem.at[peer])
        if n >= weights - 2:
            for _ in range(2):
                feed(fed)
                fed += 1
    lines(rest[weights])
    ahead(weights + AHEAD)
    sides(rest[weights - 1])
    for piece in range(fed, len(starts)):
        feed(piece)
    lines(rest[weights + 1])

    block = width // halves
    cols = sp_size // 2 * block
    y = lax.rem(sp, 2)
    down_tile = part.shape[-1]
    tiles = cols // down_tile
    in_tile = down_tile // block
    own_tile = lax.div(lax.div(sp, 2), in_tile)

    def project(side, half, tile):
        start = half * cols + tile * down_tile
        lanes = pl.ds(pl.multiple_of(start, down_tile), down_tile)
        out = jnp.dot(hidden[...], down_all[side, :, lanes], preferred_element_type=jnp.float32)
        part[side, half, tile] = out.astype(jnp.bfloat16)

    def give(side, half, order, mask, to, landing):
        def spec():
            return (
                part.at[side, half, :, rows_of(flip_bits(member, mask))],
                part_in.at[side, landing, half],
                part_out.at[side, mask, order],
                part_sem.at[side, landing, half, 0],
                2 * (to & 1),
                to & ~1,
            )

        send(None, spec)

    def give_tile(half, tile, order):
        for m in range(1, tp_size):

            def spec(m=m):
                return (
                    part.at[1, half, tile, rows_of(flip_bits(member, m))],
                    part_in.at[1, m - 1, half, tile],
                    part_out.at[1, m, order],
                    part_sem.at[1, m - 1, half, tile],
                    2 * (m & 1),
                    m & ~1,
                )

            send(None, spec)

    def give_up(side, half, low_first):
        if low_first:
            for high in range(0, tp_size, 2):
                give(side, half, 1, high + 1, 1, high)
        else:
            for m in range(2, tp_size, 2):
                for low_mask in range(2):
                    give(side, half, 0, m + low_mask, m, m + low_mask - 1)

    def give_down(side, half, low_first, bank):
        if low_first:
            jobs = [(m, [m], m, m - 1) for m in range(2, tp_size, 2)]
        else:
            jobs = [(1, list(range(2, tp_size, 2)), 1, 0)]
        for n, (mask, landings, to, landing) in enumerate(jobs):
            for m in landings:
                arrived(part_in.at[side, m, half], part_sem.at[side, m, half, 0])
            for tile in range(tiles):
                total = part[side, half, tile, rows_of(flip_bits(member, mask)), :].astype(jnp.float32)
                for m in landings:
                    total = total + part_in[side, m, half, tile].astype(jnp.float32)
                sums[bank + n, tile] = total.astype(jnp.bfloat16)

            def spec(bank=bank + n, to=to, landing=landing):
                return (
                    sums.at[bank],
                    part_in.at[side, landing, half],
                    sum_out.at[bank],
                    part_sem.at[side, landing, half, 0],
                    2 * (to & 1),
                    to & ~1,
                )

            send(None, spec)

    def finish(side, half, landings, tile):
        total = part[side, half, tile, rows_of(member), :].astype(jnp.float32)
        for landing in landings:
            total = total + part_in[side, landing, half, tile].astype(jnp.float32)
        for n in range(in_tile):
            start = (2 * (tile * in_tile + n) + half) * width + side * block
            there = pl.ds(pl.multiple_of(start, block), block)
            out_ref[:, there] = (
                updated[:, there].astype(jnp.float32) + 0.5 * total[:, n * block : (n + 1) * block]
            ).astype(out_ref.dtype)

    def finish_half(side, half, landings):
        for landing in landings:
            arrived(part_in.at[side, landing, half], part_sem.at[side, landing, half, 0])
        for tile in range(tiles):
            finish(side, half, landings, tile)

    everyone = list(range(tp_size - 1))
    for tile in range(tiles):
        project(0, y, tile)
    give_up(0, y, False)
    sides(rest[weights])
    lines(rest[weights + 2])
    sides(rest[weights + 1])
    for tile in range(tiles):
        project(0, 1 - y, tile)
    give_up(0, 1 - y, True)
    lines(rest[weights + 3])
    for tile in range(tiles):
        project(1, y, tile)
    give_up(1, y, False)
    give_down(0, y, False, 0)
    sides(rest[weights + 2])
    last = len(pending)
    for t in range(tiles):
        tile = flip_bits(own_tile, t)
        first = 2 * in_tile * t
        sides(rest[weights + 3], [m for m in across if first <= m < first + 2 * in_tile])
        project(1, 1 - y, tile)
        give_tile(1 - y, tile, 1 + t)
        if t == 0:
            give_down(0, 1 - y, True, 1)
    give_down(1, y, False, tp_size // 2)
    drain_weights()
    drain(0, last)
    kept = [0] + [m - 1 for m in range(2, tp_size, 2)]
    finish_half(0, y, kept)
    finish_half(0, 1 - y, kept)
    for t in range(tiles):
        tile = flip_bits(own_tile, t)
        for landing in everyone:
            arrived(part_in.at[1, landing, 1 - y, tile], part_sem.at[1, landing, 1 - y, tile])
        finish(1, 1 - y, everyone, tile)
    finish_half(1, y, kept)
    drain(last, len(pending))


def grid_tables(rows, head_dim):
    quarter = head_dim // 4
    frequency = np.power(theta_base, -2.0 * np.arange(quarter) / (head_dim // 2)).astype(np.float32)

    def halves(count, first):
        angle = np.arange(count, dtype=np.float32)[:, None] * frequency
        cosine, sine = np.cos(angle.astype(np.float64)), np.sin(angle.astype(np.float64))
        empty = np.zeros((count, 2 * quarter))
        both = [np.concatenate([cosine, cosine], 1), np.concatenate([-sine, sine], 1)]
        return [
            np.concatenate([b, empty] if first else [empty, b], 1).astype(np.float32) for b in both
        ]

    return halves(rows, True) + halves(GRID, False)


def fused_device(
    sp_size,
    tp_size,
    query_rows,
    key_rows,
    value_rows,
    query_gain,
    key_gain,
    residual,
    out_weight,
    mix_gain,
    gate_weight,
    up_weight,
    down_weight,
):
    tok_rows, head_dim = key_rows.shape
    own = tok_rows // tp_size
    tokens = sp_size * tok_rows
    depth, units = gate_weight.shape
    model = mix_gain.shape[0]
    width = down_weight.shape[1]
    q_width = query_rows.shape[1]
    down_tile = min(256, sp_size * width // 4)
    tiles = sp_size * width // 4 // down_tile
    tables = grid_tables(tokens // GRID, head_dim)
    any_spec = pl.BlockSpec(memory_space=pltpu.HBM)
    vmem_spec = pl.BlockSpec(memory_space=pltpu.VMEM)
    dma = pltpu.SemaphoreType.DMA
    bf16 = jnp.bfloat16
    chunk_count = 2 + 2 * pl.cdiv(units, UNIT_TILE) + 4
    vm = pltpu.VMEM
    return pl.pallas_call(
        functools.partial(layer_body, sp_size, tp_size),
        out_shape=jax.ShapeDtypeStruct(residual.shape, residual.dtype),
        in_specs=[any_spec] * 3
        + [vmem_spec] * 2
        + [any_spec] * 2
        + [vmem_spec]
        + [any_spec] * 3
        + [vmem_spec] * 4,
        out_specs=vmem_spec,
        scratch_shapes=[
            vm((tokens, head_dim), bf16),
            vm((tokens, head_dim), bf16),
            vm((tokens, head_dim), bf16),
            vm((tp_size, own, q_width), bf16),
            vm((tok_rows * q_width // head_dim, head_dim), bf16),
            vm((tp_size * out_weight.shape[0], model), bf16),
            vm((sp_size * depth, units), bf16),
            vm((sp_size * depth, units), bf16),
            vm((2, units, sp_size * width // 2), bf16),
            vm((tok_rows, q_width), bf16),
            vm((tp_size, own, q_width), bf16),
            vm((own, model), bf16),
            vm((own, model), bf16),
            vm((tok_rows, model), bf16),
            vm((tok_rows, units), bf16),
            vm((2, 2, tiles, tok_rows, down_tile), bf16),
            vm((2, tp_size - 1, 2, tiles, own, down_tile), bf16),
            vm((1 + tp_size // 2, tiles, own, down_tile), bf16),
            dma,
            dma((tp_size,)),
            dma((tp_size,)),
            dma((chunk_count, sp_size)),
            dma((5,)),
            dma((5,)),
            dma((5,)),
            dma((tp_size,)),
            dma((tp_size,)),
            dma((tp_size,)),
            dma((tp_size,)),
            dma((tp_size,)),
            dma((tp_size,)),
            dma((tp_size,)),
            dma((2, tp_size - 1, 2, tiles)),
            dma((2, tp_size, 1 + tiles)),
            dma((1 + tp_size // 2,)),
        ],
        compiler_params=pltpu.CompilerParams(
            collective_id=0, has_side_effects=True, vmem_limit_bytes=VMEM_LIMIT
        ),
    )(
        query_rows,
        key_rows,
        value_rows,
        query_gain.reshape(1, -1),
        key_gain.reshape(1, -1),
        residual,
        out_weight,
        mix_gain.reshape(1, -1),
        gate_weight,
        up_weight,
        down_weight,
        *tables,
    )


def on_any_device(sp_size, tp_size, *args):
    query_rows, key_rows, _, query_gain, _, residual, _, _, gate_weight, _, down_weight = args
    lanes = query_gain.shape[0]
    tok_rows = key_rows.shape[0]
    whole = (
        key_rows.shape[1] == lanes
        and (down_weight.shape[1] // 2) % lanes == 0
        and gate_weight.shape[1] % lanes == 0
        and (tok_rows // tp_size) % GRID == 0
        and sp_size % 4 == 0
        and tp_size % 2 == 0
    )
    device = fused_device if whole else on_device
    return device(sp_size, tp_size, *args)


def solution(mesh):
    placed = (
        P("sp", "tp"),
        P("sp", "tp"),
        P("sp", "tp"),
        P(),
        P(),
        P(("sp", "tp"), None),
        P("tp", None),
        P(),
        P("sp", "tp"),
        P("sp", "tp"),
        P("tp", "sp"),
    )
    return jax.shard_map(
        functools.partial(on_any_device, mesh.shape["sp"], mesh.shape["tp"]),
        mesh=mesh,
        in_specs=placed,
        out_specs=P(("sp", "tp"), None),
        check_vma=False,
    )
```

```python
import functools
import math

import jax
import jax.numpy as jnp
import numpy as np
from jax import lax
from jax.experimental import pallas as pl
from jax.experimental.pallas import tpu as pltpu
from jax.sharding import PartitionSpec as P

GRID = 64

norm_eps = 1e-06
theta_base = 10000.0


def spin(halfway, angles):
    cosine = jnp.cos(angles)[:, None, :]
    sine_val = jnp.sin(angles)[:, None, :]
    quarter = halfway.shape[-1] // 2
    leading = halfway[..., :quarter]
    trailing = halfway[..., quarter:]
    return [leading * cosine - trailing * sine_val, trailing * cosine + leading * sine_val]


def rotate_grid(vectors, positions):
    head_dim = vectors.shape[-1]
    quarter = head_dim // 4
    frequency = jnp.power(
        theta_base, -2.0 * jnp.arange(quarter, dtype=jnp.float32) / (head_dim // 2)
    )
    row_angle = (positions // GRID).astype(jnp.float32)[:, None] * frequency
    col_angle = (positions % GRID).astype(jnp.float32)[:, None] * frequency
    lower_half = vectors[..., : 2 * quarter]
    upper_half = vectors[..., 2 * quarter :]
    return jnp.concatenate(spin(lower_half, row_angle) + spin(upper_half, col_angle), axis=-1)


def prepare_heads(raw_heads, head_gain, positions):
    floated = raw_heads.astype(jnp.float32)
    scaled = floated * lax.rsqrt(jnp.mean(floated * floated, axis=-1, keepdims=True) + norm_eps)
    return rotate_grid(scaled * head_gain, positions).astype(jnp.bfloat16)


def row_norm(row_data, row_gain):
    floated = row_data.astype(jnp.float32)
    scaled = floated * lax.rsqrt(jnp.mean(floated * floated, axis=-1, keepdims=True) + norm_eps)
    return (scaled * row_gain).astype(jnp.bfloat16)


def attend_body(factor, q_ref, k_ref, v_ref, o_ref):
    scores = lax.dot_general(
        q_ref[0], k_ref[0], (((1,), (1,)), ((), ())), preferred_element_type=jnp.float32
    )
    top = jnp.max(scores, axis=-1, keepdims=True)
    weights = jnp.exp2((scores - top) * factor)
    total = jnp.sum(weights, axis=-1, keepdims=True)
    mixed = jnp.dot(weights.astype(jnp.bfloat16), v_ref[0], preferred_element_type=jnp.float32)
    o_ref[0] = (mixed / total).astype(o_ref.dtype)


def attend(q_stack, keys, values):
    local_kv, rows, head_dim = q_stack.shape
    count = keys.shape[1]
    tile = min(256, rows)
    return pl.pallas_call(
        functools.partial(attend_body, head_dim**-0.5 * math.log2(math.e)),
        grid=(local_kv, rows // tile),
        in_specs=[
            pl.BlockSpec((1, tile, head_dim), lambda h, i: (h, i, 0)),
            pl.BlockSpec((1, count, head_dim), lambda h, i: (h, 0, 0)),
            pl.BlockSpec((1, count, head_dim), lambda h, i: (h, 0, 0)),
        ],
        out_specs=pl.BlockSpec((1, tile, head_dim), lambda h, i: (h, i, 0)),
        out_shape=jax.ShapeDtypeStruct((local_kv, rows, head_dim), jnp.bfloat16),
        compiler_params=pltpu.CompilerParams(vmem_limit_bytes=40 * 1024 * 1024),
        cost_estimate=pl.CostEstimate(
            flops=4 * local_kv * rows * count * head_dim,
            bytes_accessed=4 * local_kv * (rows + count) * head_dim,
            transcendentals=local_kv * rows * count,
        ),
    )(q_stack, keys, values)


def on_device(
    sp_size,
    tp_size,
    query_rows,
    key_rows,
    value_rows,
    query_gain,
    key_gain,
    residual,
    out_weight,
    mix_gain,
    gate_weight,
    up_weight,
    down_weight,
):
    ring = list(range(0, sp_size, 2)) + list(range(1, sp_size, 2))[::-1]
    onward = [(ring[i], ring[(i + 1) % sp_size]) for i in range(sp_size)]
    backward = [(b, a) for a, b in onward]
    sp_index, tp_index = lax.axis_index("sp"), lax.axis_index("tp")

    def travel(piece, perm, steps):
        out = []
        for _ in range(steps):
            piece = lax.ppermute(piece, "sp", perm)
            out.append(piece)
        return out

    def relabel(piece, rule):
        perm = []
        for s in range(sp_size):
            for t in range(tp_size):
                new_s, new_t = rule(s, t)
                if (new_s, new_t) == (s, t):
                    continue
                perm.append((s * tp_size + t, new_s * tp_size + new_t))
        return lax.ppermute(piece, ("sp", "tp"), perm)

    def flip(piece, sp_mask, tp_mask):
        return relabel(piece, lambda s, t: (s ^ sp_mask, t ^ tp_mask))

    def swap_bits(s, t):
        return (s & ~2) | ((t & 1) << 1), (t & ~1) | ((s >> 1) & 1)

    tok_rows = query_rows.shape[0]
    head_dim = query_gain.shape[0]
    local_kv = key_rows.shape[1] // head_dim
    local_q = query_rows.shape[1] // head_dim
    group_size = local_q // local_kv
    positions = lax.axis_index("sp") * tok_rows + jnp.arange(tok_rows, dtype=jnp.int32)

    k_heads = prepare_heads(
        key_rows.reshape(tok_rows, local_kv, head_dim), key_gain, positions
    ).reshape(tok_rows, local_kv * head_dim)
    kv = jnp.concatenate([k_heads, value_rows], axis=1)
    far = sp_size // 2
    kv_all = [kv] + travel(kv, onward, far) + travel(kv, backward, sp_size - 1 - far)

    bits = [1 << i for i in range(sp_size.bit_length() - 1)]
    order = bits[2:][::-1] + [1, 2]

    def collect(shard, gate_on):
        swapped = relabel(shard, swap_bits)
        keeps = ((sp_index >> 1) & 1) == (tp_index & 1)
        shard = jnp.where(keeps, shard, swapped)
        if gate_on is not None:
            shard, _ = lax.optimization_barrier((shard, gate_on))
        pieces = {0: shard}
        for bit in order:
            for mask in list(pieces):
                if bit == 2:
                    pieces[mask | bit] = flip(pieces[mask], 0, 1)
                else:
                    pieces[mask | bit] = flip(pieces[mask], bit, 0)
        return [pieces[mask] for mask in range(sp_size)]

    gate_on = (kv_all[far][:8], kv_all[-1][:8])
    gate_whole = jnp.concatenate(collect(gate_weight, gate_on), axis=0)
    up_whole = jnp.concatenate(collect(up_weight, gate_on), axis=0)
    down_whole = jnp.concatenate(collect(down_weight, gate_on), axis=1)

    q_heads = prepare_heads(query_rows.reshape(tok_rows, local_q, head_dim), query_gain, positions)
    q_stack = (
        q_heads.reshape(tok_rows, local_kv, group_size, head_dim)
        .transpose(1, 2, 0, 3)
        .reshape(local_kv, group_size * tok_rows, head_dim)
    )
    kv_whole = jnp.concatenate(kv_all, axis=0)
    kv_heads = kv_whole.reshape(sp_size * tok_rows, 2, local_kv, head_dim).transpose(1, 2, 0, 3)
    attended = attend(q_stack, kv_heads[0], kv_heads[1])
    attended = (
        attended.reshape(local_kv, group_size, tok_rows, head_dim)
        .transpose(2, 0, 1, 3)
        .reshape(tok_rows, local_q * head_dim)
    )
    own_count = tok_rows // tp_size
    by_peer = [
        lax.dynamic_slice_in_dim(attended, (tp_index ^ d) * own_count, own_count, 0)
        for d in range(tp_size)
    ]

    def summed(parts, masks):
        total = parts[0].astype(jnp.float32)
        arrived = [flip(piece, *mask) for piece, mask in zip(parts[1:], masks)]
        for piece in arrived:
            total = total + piece.astype(jnp.float32)
        return total

    def row_blocks(array):
        return [array[d * own_count : (d + 1) * own_count] for d in range(tp_size)]

    base = (sp_index & ~2) | ((tp_index & 1) << 1)
    width = down_weight.shape[1]

    def reorder(array):
        return jnp.concatenate(
            [
                lax.dynamic_slice_in_dim(array, (base ^ mask) * width, width, 1)
                for mask in range(sp_size)
            ],
            axis=1,
        )

    head_part = jnp.dot(
        jnp.concatenate(by_peer, axis=0), out_weight, preferred_element_type=jnp.float32
    ).astype(jnp.bfloat16)
    attn_sum = summed(row_blocks(head_part), [(0, d) for d in range(1, tp_size)])
    own_rows = (residual.astype(jnp.float32) + attn_sum).astype(jnp.bfloat16)
    group = [(0, 2), (2, 0), (2, 2)]
    normed = reorder(row_norm(own_rows, mix_gain))
    normed_all = jnp.concatenate([normed] + [flip(normed, *mask) for mask in group], axis=0)
    gate_act = jnp.dot(normed_all, gate_whole, preferred_element_type=jnp.float32)
    up_act = jnp.dot(normed_all, up_whole, preferred_element_type=jnp.float32)
    hidden = lax.optimization_barrier((jax.nn.silu(gate_act) * up_act).astype(jnp.bfloat16))
    unit_part = jnp.dot(hidden, down_whole, preferred_element_type=jnp.float32).astype(
        jnp.bfloat16
    )
    unit_sum = reorder(summed(row_blocks(unit_part), group))
    return (own_rows.astype(jnp.float32) + 0.5 * unit_sum).astype(jnp.bfloat16)


MESH = pl.DeviceIdType.MESH
AHEAD = 6
FIRST = 3
SECOND = 10
UNIT_TILE = 256
VMEM_LIMIT = 63 * 1024 * 1024


def flip_bits(index, mask):
    out, step = index, 1
    while step <= mask:
        if mask & step:
            out = out + step * (1 - 2 * lax.rem(lax.div(index, step), 2))
        step *= 2
    return out


def turn(rows, gain, cosine, sine):
    count, head_dim = rows.shape
    quarter = head_dim // 4
    scaled = rows * lax.rsqrt(jnp.mean(rows * rows, axis=-1, keepdims=True) + norm_eps) * gain
    lane = lax.broadcasted_iota(jnp.int32, (count, head_dim), 1)
    paired = jnp.where(
        lax.rem(lane, 2 * quarter) < quarter,
        pltpu.roll(scaled, head_dim - quarter, 1),
        pltpu.roll(scaled, quarter, 1),
    )
    turned = scaled.reshape(cosine.shape) * cosine + paired.reshape(cosine.shape) * sine
    return turned.reshape(count, head_dim).astype(jnp.bfloat16)


def layer_body(
    sp_size,
    tp_size,
    q_ref,
    k_ref,
    v_ref,
    q_gain_ref,
    k_gain_ref,
    res_ref,
    ow_ref,
    mix_ref,
    gate_ref,
    up_ref,
    down_ref,
    row_cos_ref,
    row_sin_ref,
    col_cos_ref,
    col_sin_ref,
    out_ref,
    k_raw,
    v_all,
    k_all,
    q_raw,
    q_all,
    ow_all,
    gate_all,
    up_all,
    down_all,
    att,
    att_in,
    res,
    updated,
    normed,
    hidden,
    part,
    part_in,
    sums,
    copy_sem,
    q_sem,
    q_out,
    w_sem,
    z_out,
    y_out,
    d_out,
    ow_sem,
    ow_out,
    ow_on,
    att_sem,
    att_out,
    norm_sem,
    norm_out,
    part_sem,
    part_out,
    sum_out,
):
    sp, tp = lax.axis_index("sp"), lax.axis_index("tp")
    core = lax.rem(tp, 2)
    low = lax.rem(lax.div(sp, 2), 2)
    member = tp - core + low
    at_home = low == core
    tok_rows, head_dim = k_ref.shape
    own = tok_rows // tp_size
    heads = q_ref.shape[1] // head_dim
    depth, units = gate_ref.shape
    width = down_ref.shape[1]
    model = mix_ref.shape[1]
    group_rows = own * tp_size
    line = [m for m in range(2, sp_size, 2)]
    across = [m for m in range(1, sp_size, 2)]
    far = [m for m in range(4, sp_size, 4)]
    near = [m for m in range(2, sp_size, 4)]
    pending = []

    def remote(src, dst, out_sem, in_sem, sp_mask, tp_mask):
        return pltpu.make_async_remote_copy(
            src_ref=src,
            dst_ref=dst,
            send_sem=out_sem,
            recv_sem=in_sem,
            device_id=(flip_bits(sp, sp_mask), flip_bits(tp, tp_mask)),
            device_id_type=MESH,
        )

    def send(where, spec):
        remote(*spec()).start()
        pending.append((where, spec))

    def drain(first, stop):
        def of(kind):
            for where, spec in pending[first:stop]:
                if where == kind:
                    remote(*spec()).wait_send()

        of(None)
        pl.when(at_home)(lambda: of("home"))
        pl.when(jnp.logical_not(at_home))(lambda: of("away"))

    def arrived(dst, sem):
        pltpu.make_async_copy(dst, dst, sem).wait()

    friends = (
        [(m, 0) for m in line]
        + [(1, 0), (0, 1), (2, 1)]
        + [(2 * (m & 1), m & ~1) for m in range(2, tp_size)]
    )
    barrier = pltpu.get_barrier_semaphore()
    for sp_mask, tp_mask in friends:
        pl.semaphore_signal(
            barrier,
            inc=1,
            device_id=(flip_bits(sp, sp_mask), flip_bits(tp, tp_mask)),
            device_id_type=MESH,
        )

    halves = 2
    chunks = [("k", 0, 0), ("v", 0, 0)]
    starts = list(range(0, units, UNIT_TILE))
    for start in starts:
        chunks += [("g", start, 0), ("u", start, 0)]
    for side in range(halves):
        for half in range(halves):
            chunks.append(("d", half, side))
    place = {name: i for i, name in enumerate(chunks)}

    def source(chunk):
        kind, half, side = chunk
        if kind in "kv":
            return k_ref if kind == "k" else v_ref
        if kind in "gu":
            ref = gate_ref if kind == "g" else up_ref
            return ref.at[:, pl.ds(half, min(UNIT_TILE, units - half))]
        return down_ref.at[
            pl.ds(half * (units // halves), units // halves),
            pl.ds(side * (width // halves), width // halves),
        ]

    def slot(chunk, shard):
        kind, half, side = chunk
        if kind in "kv":
            ref = k_raw if kind == "k" else v_all
            return ref.at[pl.ds(pl.multiple_of(shard * tok_rows, tok_rows), tok_rows)]
        if kind in "gu":
            ref = gate_all if kind == "g" else up_all
            rows = pl.ds(pl.multiple_of(shard * depth, depth), depth)
            return ref.at[rows, pl.ds(half, min(UNIT_TILE, units - half))]
        cols = width // halves
        rows = units // halves
        place_of = lax.rem(shard, 2) * (sp_size // 2) + lax.div(shard, 2)
        return down_all.at[
            side, pl.ds(half * rows, rows), pl.ds(pl.multiple_of(place_of * cols, cols), cols)
        ]

    def bank(chunk):
        return "kvgud".index(chunk[0])

    def push(src, dst, out_sem, in_sem, sp_mask, tp_mask):
        remote(src, dst, out_sem, in_sem, sp_mask, tp_mask).start()

    def along(chunk):
        n = place[chunk]
        src, dst, sem = source(chunk), slot(chunk, sp), w_sem.at[n, sp]

        @pl.when(at_home)
        def _():
            for mask in far:
                push(src, dst, z_out.at[bank(chunk)], sem, mask, 0)

        @pl.when(jnp.logical_not(at_home))
        def _():
            for mask in near:
                push(src, dst, z_out.at[bank(chunk)], sem, mask, 0)

    def settle(chunk):
        pltpu.make_async_copy(source(chunk), slot(chunk, sp), w_sem.at[place[chunk], sp]).start()

    def offer(chunk):
        n = place[chunk]
        src, dst, sem = source(chunk), slot(chunk, sp), w_sem.at[n, sp]

        @pl.when(at_home)
        def _():
            push(src, dst, y_out.at[bank(chunk)], sem, 1, 0)
            push(src, dst, d_out.at[bank(chunk)], sem, 0, 1)

    def relay(chunk, masks, over):
        n = place[chunk]
        for mask in masks:
            shard = flip_bits(sp, mask)
            here, sem = slot(chunk, shard), w_sem.at[n, shard]
            arrived(here, sem)

            @pl.when(at_home)
            def _():
                if over:
                    push(here, here, y_out.at[bank(chunk)], sem, 1, 0)
                push(here, here, d_out.at[bank(chunk)], sem, 0, 1)

    def lines(chunk):
        relay(chunk, line, True)
        arrived(slot(chunk, sp), w_sem.at[place[chunk], sp])

    def sides(chunk, masks=across):
        relay(chunk, masks, False)

    def drain_weights():
        def spans(count):
            for name, ref in enumerate((k_raw, v_all)):
                yield name, ref.at[pl.ds(0, count * tok_rows)]
            for name, ref in enumerate((gate_all, up_all)):
                yield 2 + name, ref.at[pl.ds(0, count * depth)]
            yield 4, down_all.at[:, :, pl.ds(0, count * (width // halves))]

        def wait(sem, count):
            for name, ref in spans(count):
                arrived(ref, sem.at[name])

        @pl.when(at_home)
        def _():
            if far:
                wait(z_out, len(far))
            wait(y_out, len(line) + 1)
            wait(d_out, sp_size)

        @pl.when(jnp.logical_not(at_home))
        def _():
            wait(z_out, len(near))

    res_copy = pltpu.make_async_copy(res_ref, res, copy_sem)
    res_copy.start()
    ow_rows = ow_ref.shape[0]

    def ow_slot(index):
        return ow_all.at[pl.ds(pl.multiple_of(index * ow_rows, ow_rows), ow_rows)]

    pltpu.make_async_copy(ow_ref, ow_slot(tp), ow_sem.at[tp]).start()

    @pl.when(at_home)
    def _():
        for chunk in chunks:
            settle(chunk)

    pl.semaphore_wait(barrier, len(friends))

    for hi in range(tp_size // 2):
        for rel in range(2):

            def spec(sp_mask, tp_mask, hi=hi, rel=rel):
                mate = core + rel - 2 * core * rel
                src = q_ref.at[pl.ds(pl.multiple_of((2 * hi + mate) * own, own), own)]
                dst, sem = q_raw.at[2 * hi + low], q_sem.at[2 * hi + low]
                return src, dst, q_out.at[2 * hi + rel], sem, sp_mask, tp_mask

            @pl.when(at_home)
            def _():
                if rel == 0:
                    src, dst, _, sem, _, _ = spec(0, 0)
                    pltpu.make_async_copy(src, dst, sem).start()
                else:
                    send("home", lambda spec=spec: spec(0, 1))

            @pl.when(jnp.logical_not(at_home))
            def _():
                send("away", lambda spec=spec, rel=rel: spec(2, rel))

    kv = chunks[:2]
    rest = chunks[2:]
    for chunk in kv:
        along(chunk)
        offer(chunk)
    for hi in range(2, tp_size, 2):
        send(None, lambda hi=hi: (ow_ref, ow_slot(tp), ow_out.at[hi], ow_sem.at[tp], 0, hi))
    send(None, lambda: (ow_ref, ow_slot(tp), ow_out.at[0], ow_sem.at[tp], 0, 1))
    along(rest[0])
    for n in range(FIRST):
        offer(rest[n])

    def ahead(n):
        if n < len(rest):
            along(rest[n])

    row_count = tok_rows // GRID

    def table(ref, col_ref, start, count):
        return ref[pl.ds(start, count), :][:, None, :] + col_ref[...][None]

    for m in range(tp_size):
        arrived(q_raw.at[m], q_sem.at[m])
        their_sp = sp - 2 * low + 2 * (m % 2)
        their_tp = 2 * (m // 2) + core
        own_grid = own // GRID
        start = (their_sp * tp_size + their_tp) * own_grid
        cosine = table(row_cos_ref, col_cos_ref, start, own_grid)
        sine = table(row_sin_ref, col_sin_ref, start, own_grid)
        for h in range(heads):
            raw = q_raw[m, :, h * head_dim : (h + 1) * head_dim].astype(jnp.float32)
            q_all[pl.ds(h * group_rows + m * own, own), :] = turn(
                raw, q_gain_ref[...], cosine, sine
            )

    def ready_keys(masks):
        for mask in masks:
            shard = flip_bits(sp, mask)
            rows = pl.ds(pl.multiple_of(shard * tok_rows, tok_rows), tok_rows)
            start = pl.multiple_of(shard * row_count, row_count)
            k_all[rows, :] = turn(
                k_raw[rows, :].astype(jnp.float32),
                k_gain_ref[...],
                table(row_cos_ref, col_cos_ref, start, row_count),
                table(row_sin_ref, col_sin_ref, start, row_count),
            )

    for chunk in kv:
        lines(chunk)
    for n in range(FIRST, SECOND):
        offer(rest[n])
    for n in range(1, AHEAD):
        along(rest[n])
    ready_keys(line)
    for chunk in kv:
        sides(chunk)
    ready_keys([0] + across)

    for hi in range(2, tp_size, 2):
        block = ow_slot(flip_bits(tp, hi))
        arrived(block, ow_sem.at[flip_bits(tp, hi)])

        def spec(hi=hi):
            index = flip_bits(tp, hi)
            return ow_slot(index), ow_slot(index), ow_on.at[hi], ow_sem.at[index], 0, 1

        send(None, spec)
    lines(rest[0])

    factor = head_dim**-0.5 * math.log2(math.e)
    tile = min(256, group_rows)
    per_head = group_rows // tile

    def attend_tile(i, carry):
        q_tile = q_all[pl.ds(pl.multiple_of(i * tile, tile), tile), :]
        scores = lax.dot_general(
            q_tile, k_all[...], (((1,), (1,)), ((), ())), preferred_element_type=jnp.float32
        )
        top = jnp.max(scores, axis=-1, keepdims=True)
        weights = jnp.exp2((scores - top) * factor)
        total = jnp.sum(weights, axis=-1, keepdims=True)
        mixed = jnp.dot(
            weights.astype(jnp.bfloat16), v_all[...], preferred_element_type=jnp.float32
        )
        head = lax.div(i, per_head)
        start = pl.multiple_of(lax.rem(i, per_head) * tile, tile)
        lanes = pl.ds(pl.multiple_of(head * head_dim, head_dim), head_dim)
        att[pl.ds(start, tile), lanes] = (mixed / total).astype(att.dtype)
        return carry

    lax.fori_loop(0, heads * per_head, attend_tile, 0)

    def rows_of(index):
        return pl.ds(pl.multiple_of(index * own, own), own)

    for m in range(1, tp_size):
        send(
            None,
            lambda m=m: (
                att.at[rows_of(flip_bits(member, m))],
                att_in.at[member],
                att_out.at[m],
                att_sem.at[member],
                2 * (m & 1),
                m & ~1,
            ),
        )
    att_in[member] = att[rows_of(member), :]

    lines(rest[1])
    for n in range(SECOND, len(rest)):
        offer(rest[n])
    sides(rest[0])
    lines(rest[2])
    sides(rest[1])
    arrived(ow_slot(tp), ow_sem.at[tp])
    for hi in range(0, tp_size, 2):
        index = flip_bits(tp, hi + 1)
        arrived(ow_slot(index), ow_sem.at[index])
    res_copy.wait()
    for m in range(1, tp_size):
        arrived(att_in.at[flip_bits(member, m)], att_sem.at[flip_bits(member, m)])

    column = min(512, model)
    for start in range(0, model, column):
        lanes = slice(start, start + column)
        total = res[:, lanes].astype(jnp.float32)
        summed = None
        for m in range(tp_size):
            piece = (
                jnp.dot(
                    att_in[m],
                    ow_all[m * ow_rows : (m + 1) * ow_rows, lanes],
                    preferred_element_type=jnp.float32,
                )
                .astype(jnp.bfloat16)
                .astype(jnp.float32)
            )
            summed = piece if summed is None else summed + piece
        updated[:, lanes] = (total + summed).astype(jnp.bfloat16)
    floated = updated[...].astype(jnp.float32)
    scale = lax.rsqrt(jnp.mean(floated * floated, axis=-1, keepdims=True) + norm_eps)
    normed[rows_of(member), :] = (floated * scale * mix_ref[...]).astype(jnp.bfloat16)

    def normed_spec(index, out_sem, mask):
        rows = normed.at[rows_of(index)]
        return rows, rows, out_sem, norm_sem.at[index], 2 * (mask & 1), mask & ~1

    for m in [1] + list(range(2, tp_size, 2)):
        send(None, lambda m=m: normed_spec(member, norm_out.at[m], m))

    def normed_on():
        mate = flip_bits(member, 1)
        arrived(normed.at[rows_of(mate)], norm_sem.at[mate])
        for m in range(2, tp_size, 2):
            send(None, lambda m=m: normed_spec(flip_bits(member, 1), norm_out.at[m + 1], m))

    def feed(piece):
        lanes = slice(starts[piece], min(starts[piece] + UNIT_TILE, units))
        gate = jnp.dot(normed[...], gate_all[:, lanes], preferred_element_type=jnp.float32)
        up = jnp.dot(normed[...], up_all[:, lanes], preferred_element_type=jnp.float32)
        hidden[:, lanes] = (gate / (1.0 + jnp.exp(-gate)) * up).astype(jnp.bfloat16)

    weights = 2 * len(starts)
    fed = 0
    for n in range(AHEAD, AHEAD + 3):
        ahead(n)
    for n in range(3, weights):
        lines(rest[n])
        ahead(n + AHEAD)
        sides(rest[n - 1])
        if n == weights // 2:
            normed_on()
        if n == weights - 2:
            for m in range(2, tp_size):
                peer = flip_bits(member, m)
                arrived(normed.at[rows_of(peer)], norm_sem.at[peer])
        if n >= weights - 2:
            for _ in range(2):
                feed(fed)
                fed += 1
    lines(rest[weights])
    ahead(weights + AHEAD)
    sides(rest[weights - 1])
    for piece in range(fed, len(starts)):
        feed(piece)
    lines(rest[weights + 1])

    block = width // halves
    cols = sp_size // 2 * block
    y = lax.rem(sp, 2)
    down_tile = part.shape[-1]
    tiles = cols // down_tile
    in_tile = down_tile // block
    own_tile = lax.div(lax.div(sp, 2), in_tile)

    def project(side, half, tile):
        start = half * cols + tile * down_tile
        lanes = pl.ds(pl.multiple_of(start, down_tile), down_tile)
        out = jnp.dot(hidden[...], down_all[side, :, lanes], preferred_element_type=jnp.float32)
        part[side, half, tile] = out.astype(jnp.bfloat16)

    def give(side, half, order, mask, to, landing):
        def spec():
            return (
                part.at[side, half, :, rows_of(flip_bits(member, mask))],
                part_in.at[side, landing, half],
                part_out.at[side, mask, order],
                part_sem.at[side, landing, half, 0],
                2 * (to & 1),
                to & ~1,
            )

        send(None, spec)

    def give_tile(half, tile, order):
        for m in range(1, tp_size):

            def spec(m=m):
                return (
                    part.at[1, half, tile, rows_of(flip_bits(member, m))],
                    part_in.at[1, m - 1, half, tile],
                    part_out.at[1, m, order],
                    part_sem.at[1, m - 1, half, tile],
                    2 * (m & 1),
                    m & ~1,
                )

            send(None, spec)

    def give_up(side, half, low_first):
        if low_first:
            for high in range(0, tp_size, 2):
                give(side, half, 1, high + 1, 1, high)
        else:
            for m in range(2, tp_size, 2):
                for low_mask in range(2):
                    give(side, half, 0, m + low_mask, m, m + low_mask - 1)

    def give_down(side, half, low_first, bank):
        if low_first:
            jobs = [(m, [m], m, m - 1) for m in range(2, tp_size, 2)]
        else:
            jobs = [(1, list(range(2, tp_size, 2)), 1, 0)]
        for n, (mask, landings, to, landing) in enumerate(jobs):
            for m in landings:
                arrived(part_in.at[side, m, half], part_sem.at[side, m, half, 0])
            for tile in range(tiles):
                total = part[side, half, tile, rows_of(flip_bits(member, mask)), :].astype(jnp.float32)
                for m in landings:
                    total = total + part_in[side, m, half, tile].astype(jnp.float32)
                sums[bank + n, tile] = total.astype(jnp.bfloat16)

            def spec(bank=bank + n, to=to, landing=landing):
                return (
                    sums.at[bank],
                    part_in.at[side, landing, half],
                    sum_out.at[bank],
                    part_sem.at[side, landing, half, 0],
                    2 * (to & 1),
                    to & ~1,
                )

            send(None, spec)

    def finish(side, half, landings, tile):
        total = part[side, half, tile, rows_of(member), :].astype(jnp.float32)
        for landing in landings:
            total = total + part_in[side, landing, half, tile].astype(jnp.float32)
        for n in range(in_tile):
            start = (2 * (tile * in_tile + n) + half) * width + side * block
            there = pl.ds(pl.multiple_of(start, block), block)
            out_ref[:, there] = (
                updated[:, there].astype(jnp.float32) + 0.5 * total[:, n * block : (n + 1) * block]
            ).astype(out_ref.dtype)

    def finish_half(side, half, landings):
        for landing in landings:
            arrived(part_in.at[side, landing, half], part_sem.at[side, landing, half, 0])
        for tile in range(tiles):
            finish(side, half, landings, tile)

    everyone = list(range(tp_size - 1))
    for tile in range(tiles):
        project(0, y, tile)
    give_up(0, y, False)
    sides(rest[weights])
    lines(rest[weights + 2])
    sides(rest[weights + 1])
    for tile in range(tiles):
        project(0, 1 - y, tile)
    give_up(0, 1 - y, True)
    lines(rest[weights + 3])
    for tile in range(tiles):
        project(1, y, tile)
    give_up(1, y, False)
    give_down(0, y, False, 0)
    sides(rest[weights + 2])
    last = len(pending)
    for t in range(tiles):
        tile = flip_bits(own_tile, t)
        first = 2 * in_tile * t
        sides(rest[weights + 3], [m for m in across if first <= m < first + 2 * in_tile])
        project(1, 1 - y, tile)
        give_tile(1 - y, tile, 1 + t)
        if t == 0:
            give_down(0, 1 - y, True, 1)
    give_down(1, y, False, tp_size // 2)
    drain_weights()
    drain(0, last)
    kept = [0] + [m - 1 for m in range(2, tp_size, 2)]
    finish_half(0, y, kept)
    finish_half(0, 1 - y, kept)
    for t in range(tiles):
        tile = flip_bits(own_tile, t)
        for landing in everyone:
            arrived(part_in.at[1, landing, 1 - y, tile], part_sem.at[1, landing, 1 - y, tile])
        finish(1, 1 - y, everyone, tile)
    finish_half(1, y, kept)
    drain(last, len(pending))


def grid_tables(rows, head_dim):
    quarter = head_dim // 4
    frequency = np.power(theta_base, -2.0 * np.arange(quarter) / (head_dim // 2)).astype(np.float32)

    def halves(count, first):
        angle = np.arange(count, dtype=np.float32)[:, None] * frequency
        cosine, sine = np.cos(angle.astype(np.float64)), np.sin(angle.astype(np.float64))
        empty = np.zeros((count, 2 * quarter))
        both = [np.concatenate([cosine, cosine], 1), np.concatenate([-sine, sine], 1)]
        return [
            np.concatenate([b, empty] if first else [empty, b], 1).astype(np.float32) for b in both
        ]

    return halves(rows, True) + halves(GRID, False)


def fused_device(
    sp_size,
    tp_size,
    query_rows,
    key_rows,
    value_rows,
    query_gain,
    key_gain,
    residual,
    out_weight,
    mix_gain,
    gate_weight,
    up_weight,
    down_weight,
):
    tok_rows, head_dim = key_rows.shape
    own = tok_rows // tp_size
    tokens = sp_size * tok_rows
    depth, units = gate_weight.shape
    model = mix_gain.shape[0]
    width = down_weight.shape[1]
    q_width = query_rows.shape[1]
    down_tile = min(256, sp_size * width // 4)
    tiles = sp_size * width // 4 // down_tile
    tables = grid_tables(tokens // GRID, head_dim)
    any_spec = pl.BlockSpec(memory_space=pltpu.HBM)
    vmem_spec = pl.BlockSpec(memory_space=pltpu.VMEM)
    dma = pltpu.SemaphoreType.DMA
    bf16 = jnp.bfloat16
    chunk_count = 2 + 2 * pl.cdiv(units, UNIT_TILE) + 4
    vm = pltpu.VMEM
    return pl.pallas_call(
        functools.partial(layer_body, sp_size, tp_size),
        out_shape=jax.ShapeDtypeStruct(residual.shape, residual.dtype),
        in_specs=[any_spec] * 3
        + [vmem_spec] * 2
        + [any_spec] * 2
        + [vmem_spec]
        + [any_spec] * 3
        + [vmem_spec] * 4,
        out_specs=vmem_spec,
        scratch_shapes=[
            vm((tokens, head_dim), bf16),
            vm((tokens, head_dim), bf16),
            vm((tokens, head_dim), bf16),
            vm((tp_size, own, q_width), bf16),
            vm((tok_rows * q_width // head_dim, head_dim), bf16),
            vm((tp_size * out_weight.shape[0], model), bf16),
            vm((sp_size * depth, units), bf16),
            vm((sp_size * depth, units), bf16),
            vm((2, units, sp_size * width // 2), bf16),
            vm((tok_rows, q_width), bf16),
            vm((tp_size, own, q_width), bf16),
            vm((own, model), bf16),
            vm((own, model), bf16),
            vm((tok_rows, model), bf16),
            vm((tok_rows, units), bf16),
            vm((2, 2, tiles, tok_rows, down_tile), bf16),
            vm((2, tp_size - 1, 2, tiles, own, down_tile), bf16),
            vm((1 + tp_size // 2, tiles, own, down_tile), bf16),
            dma,
            dma((tp_size,)),
            dma((tp_size,)),
            dma((chunk_count, sp_size)),
            dma((5,)),
            dma((5,)),
            dma((5,)),
            dma((tp_size,)),
            dma((tp_size,)),
            dma((tp_size,)),
            dma((tp_size,)),
            dma((tp_size,)),
            dma((tp_size,)),
            dma((tp_size,)),
            dma((2, tp_size - 1, 2, tiles)),
            dma((2, tp_size, 1 + tiles)),
            dma((1 + tp_size // 2,)),
        ],
        compiler_params=pltpu.CompilerParams(
            collective_id=0, has_side_effects=True, vmem_limit_bytes=VMEM_LIMIT
        ),
    )(
        query_rows,
        key_rows,
        value_rows,
        query_gain.reshape(1, -1),
        key_gain.reshape(1, -1),
        residual,
        out_weight,
        mix_gain.reshape(1, -1),
        gate_weight,
        up_weight,
        down_weight,
        *tables,
    )


def on_any_device(sp_size, tp_size, *args):
    query_rows, key_rows, _, query_gain, _, residual, _, _, gate_weight, _, down_weight = args
    lanes = query_gain.shape[0]
    tok_rows = key_rows.shape[0]
    whole = (
        key_rows.shape[1] == lanes
        and (down_weight.shape[1] // 2) % lanes == 0
        and gate_weight.shape[1] % lanes == 0
        and (tok_rows // tp_size) % GRID == 0
        and sp_size % 4 == 0
        and tp_size % 2 == 0
    )
    device = fused_device if whole else on_device
    return device(sp_size, tp_size, *args)


def solution(mesh):
    placed = (
        P("sp", "tp"),
        P("sp", "tp"),
        P("sp", "tp"),
        P(),
        P(),
        P(("sp", "tp"), None),
        P("tp", None),
        P(),
        P("sp", "tp"),
        P("sp", "tp"),
        P("tp", "sp"),
    )
    return jax.shard_map(
        functools.partial(on_any_device, mesh.shape["sp"], mesh.shape["tp"]),
        mesh=mesh,
        in_specs=placed,
        out_specs=P(("sp", "tp"), None),
        check_vma=False,
    )
```
